128 devices in a mesh: sp: 16 (over z, y), tp: 8 (over x, core).
Axes of the slice: x: 4, y: 4, z: 4, core: 2. Of those that a mesh axis runs over, the one named last changes fastest.
Arguments:
- query_proj: bfloat16 [16384, 2048], P('sp', 'tp'), may hold values from -6 to 6
- key_proj: bfloat16 [16384, 2048], P('sp', 'tp'), may hold values from -6 to 6
- value_proj: bfloat16 [16384, 4096], P('sp', 'tp'), may hold values from -6 to 6
- gate_proj: bfloat16 [16384, 4096], P('sp', 'tp'), may hold values from -6 to 6
- log_decay: float32 [16384, 8], P('sp', 'tp'), may hold values from -0.75 to 0, as said below
- residual: bfloat16 [16384, 2048], P('sp'), may hold values from -4 to 4
- out_weight: bfloat16 [4096, 2048], P('tp'), may hold values from -0.09375 to 0.09375
- norm_gain: float32 [2, 2048], replicated, may hold values from 0.1 to 1.9
- norm_bias: float32 [2, 2048], replicated, may hold values from -1.5 to 1.5
- up_gate: bfloat16 [2048, 5632], P('sp', 'tp'), may hold values from -0.125 to 0.125
- up_value: bfloat16 [2048, 5632], P('sp', 'tp'), may hold values from -0.125 to 0.125
- conv_weight: float32 [2, 3, 5632], P(None, None, 'tp'), may hold values from -3 to 3
- conv_bias: float32 [2, 5632], P(None, 'tp'), may hold values from -1.5 to 1.5
- down_weight: bfloat16 [5632, 2048], P('tp', 'sp'), may hold values from -0.078125 to 0.078125
Outputs:
- layer_output: bfloat16 [16384, 2048], P(('sp', 'tp'))
The draws below stay inside these ranges and needn't reach their ends.
Inputs may be any that keep to these rules, and one draw needn't show every extreme that they name: `log_decay`: all entries are negative.
All inputs are finite; a program needn't handle non-finite values.
Results may differ from the reference program's by a relative error of at most 0.023.
Values may be sent and summed in bfloat16 or wider, within the bound.
No kernel may reach another device: no remote copies, remote signals or barrier semaphores. Data moves between devices by JAX's collectives and lax.ppermute only.
A program may use at most 128 MiB of HBM per device.

```python
import math
import jax
import jax.numpy as jnp
from jax import lax

D = 2048
RETENTION_HEADS = 8
DK = 256
DV = 512
FF = 5632
BLOCK = 256
TOK_DEV = 1024
SEQUENCE_TOKENS = 16384
N_TP = 8


def draw_log_decay(key, part):
    random_keys = jax.random.split(jax.random.fold_in(key, 71), 7)
    fast_limit = 5
    quick_decay_heads = jax.random.randint(random_keys[0], (RETENTION_HEADS,), 0, 10) < fast_limit
    fast_span = jax.random.uniform(random_keys[1], (RETENTION_HEADS,), jnp.float32, 30.0, 50.0)
    slow_rate = -0.2 / SEQUENCE_TOKENS * jax.random.uniform(random_keys[2], (RETENTION_HEADS,), jnp.float32, 0.5, 1.0)
    decay_base_rate = jnp.where(quick_decay_heads, -math.log(10.0) / fast_span, slow_rate)
    device_count = SEQUENCE_TOKENS // TOK_DEV
    replica_multiplier = jnp.exp(jax.random.uniform(random_keys[3], (device_count, RETENTION_HEADS), jnp.float32, math.log(0.5), math.log(2.0)))
    replica_multiplier = jnp.repeat(replica_multiplier, TOK_DEV, axis=0)
    jitter_amount = jax.random.uniform(random_keys[4], (SEQUENCE_TOKENS, RETENTION_HEADS), jnp.float32, 0.5, 1.5)
    spike_positions = jax.random.randint(random_keys[5], (2, RETENTION_HEADS), 0, SEQUENCE_TOKENS)
    spike_lengths = jax.random.uniform(random_keys[6], (2, RETENTION_HEADS), jnp.float32, math.log(0.5), math.log(0.8))
    position_slots = jnp.arange(SEQUENCE_TOKENS)[:, None]
    spike_events = jnp.where(position_slots == spike_positions[0][None, :], spike_lengths[0][None, :], 0.0)
    spike_events = spike_events + jnp.where(position_slots == spike_positions[1][None, :], spike_lengths[1][None, :], 0.0)
    spike_events = jnp.where(quick_decay_heads[None, :], 0.0, spike_events)
    return (decay_base_rate[None, :] * replica_multiplier * jitter_amount + spike_events).astype(jnp.float32)


def shard_levels(rng, extent, cuts, least, largest):
    def one(position, parts):
        steps = jax.random.uniform(jax.random.fold_in(jax.random.fold_in(rng, 6), position), (parts,), jnp.float32, least / len(cuts), largest / len(cuts))
        return jnp.repeat(jnp.exp(steps), extent[position] // parts).reshape((-1,) + (1,) * (len(extent) - position - 1))

    loudness = one(*cuts[0])
    for cut in cuts[1:]:
        loudness = loudness * one(*cut)
    return loudness


def normal_values(own_key, dims, deviation, limit, cuts=(), held_as=jnp.bfloat16):
    values = jax.random.normal(own_key, dims, jnp.float32) * deviation
    if len(cuts) > 0:
        values = shard_levels(own_key, dims, cuts, -0.22, 0.18) * values
    return jnp.clip(values, min=-limit, max=limit).astype(held_as)


def setup_inputs(seed: int = 0) -> dict:
    splits = jax.random.split(jax.random.key(seed), 15)
    query_proj = normal_values(splits[0], (SEQUENCE_TOKENS, RETENTION_HEADS * DK), 1.0, 6.0, ((0, 16), (1, 8)))
    key_proj = normal_values(splits[1], (SEQUENCE_TOKENS, RETENTION_HEADS * DK), 1.0, 6.0, ((0, 16), (1, 8)))
    value_proj = normal_values(splits[2], (SEQUENCE_TOKENS, RETENTION_HEADS * DV), 1.0, 6.0, ((0, 16), (1, 8)))
    gate_proj = normal_values(splits[3], (SEQUENCE_TOKENS, RETENTION_HEADS * DV), 1.0, 6.0, ((0, 16), (1, 8)))
    log_decay = draw_log_decay(jax.random.fold_in(splits[14], 71), 0)
    residual = normal_values(splits[5], (SEQUENCE_TOKENS, D), 0.5, 4.0, ((0, 16),))
    out_weight = normal_values(splits[6], (RETENTION_HEADS * DV, D), (RETENTION_HEADS * DV) ** -0.5, 0.09375, ((0, 8),))
    norm_gain = jnp.clip(1.0 + 0.18 * jax.random.normal(splits[7], (2, D), jnp.float32), 0.1, 1.9)
    norm_bias = normal_values(splits[8], (2, D), 0.3, 1.5, (), jnp.float32)
    up_gate = normal_values(splits[9], (D, FF), D ** -0.5, 0.125, ((0, 16), (1, 8)))
    up_value = normal_values(splits[10], (D, FF), D ** -0.5, 0.125, ((0, 16), (1, 8)))
    conv_weight = normal_values(splits[11], (2, 3, FF), 0.577, 3.0, ((2, 8),), jnp.float32)
    conv_bias = normal_values(splits[12], (2, FF), 0.3, 1.5, ((1, 8),), jnp.float32)
    down_weight = normal_values(splits[13], (FF, D), FF ** -0.5, 0.078125, ((0, 8), (1, 16)))
    return dict(query_proj=query_proj, key_proj=key_proj, value_proj=value_proj, gate_proj=gate_proj, log_decay=log_decay, residual=residual, out_weight=out_weight, norm_gain=norm_gain, norm_bias=norm_bias, up_gate=up_gate, up_value=up_value, conv_weight=conv_weight, conv_bias=conv_bias, down_weight=down_weight)


alpha_scale = 8.0 ** 0.25
rope_base = 10000.0
tiny_stabilizer = 1e-05

def rotate(vectors, positions):
    head_width = vectors.shape[-1]
    half_width = head_width // 2
    inverse_freq = rope_base ** (-2.0 * jnp.arange(half_width, dtype=jnp.float32) / head_width)
    angles = positions[:, None] * inverse_freq[None, :]
    cosine = jnp.cos(angles)[:, None, :]
    sine_part = jnp.sin(angles)[:, None, :]
    front = vectors[..., :half_width]
    second = vectors[..., half_width:]
    return jnp.concatenate([front * cosine - second * sine_part, front * sine_part + second * cosine], axis=-1)

def layer_norm(values, gain, shift):
    average = values.mean(-1, keepdims=True)
    spread = jnp.square(values - average).mean(-1, keepdims=True)
    return (values - average) * lax.rsqrt(spread + tiny_stabilizer) * gain + shift

def rounded(values):
    return lax.optimization_barrier(values.astype(jnp.bfloat16)).astype(jnp.float32)

def block_parts(query_tile, lookup_piece, payload_piece, log_blk):
    cum_log = jnp.cumsum(log_blk, axis=0)
    cum_heads = cum_log.T
    log_gap = cum_heads[:, :, None] - cum_heads[:, None, :]
    offsets = jnp.arange(log_blk.shape[0])
    causal = (offsets[:, None] >= offsets[None, :])[None]
    weight = jnp.where(causal, jnp.exp(jnp.where(causal, log_gap, 0.0)), 0.0)
    score_matrix = jnp.einsum('jka,ska->kjs', query_tile.astype(jnp.float32), lookup_piece.astype(jnp.float32))
    segment_scaling = (score_matrix * weight).astype(jnp.bfloat16)
    within = jnp.einsum('htm,mhe->the', segment_scaling.astype(jnp.float32), payload_piece.astype(jnp.float32))
    block_total = cum_log[-1]
    to_end = jnp.exp(block_total[None, :] - cum_log)
    faded_lookup_vector = rounded(lookup_piece.astype(jnp.float32) * to_end[:, :, None])
    summand_term = jnp.einsum('ajo,ajd->jod', faded_lookup_vector, payload_piece.astype(jnp.float32), precision=lax.Precision.HIGHEST)
    scaled_query = rounded(query_tile.astype(jnp.float32) * jnp.exp(cum_log)[:, :, None])
    return (within, scaled_query, summand_term, jnp.exp(block_total))

def grouped_product(left, right, group_count):
    group_width = left.shape[1] // group_count
    left_groups = left.reshape(left.shape[0], group_count, group_width).transpose(1, 0, 2)
    right_groups = right.reshape(group_count, group_width, right.shape[1])

    def add_group(total, pieces):
        term = jnp.dot(pieces[0], pieces[1], preferred_element_type=jnp.float32).astype(jnp.bfloat16)
        return (total + term.astype(jnp.float32), None)
    blank_sum = jnp.zeros((left.shape[0], right.shape[1]), jnp.float32)
    total, _ = lax.scan(add_group, blank_sum, (left_groups, right_groups))
    return total

def causal_conv(rows, taps, shift):
    padded = jnp.pad(rows.astype(jnp.float32), ((2, 0), (0, 0)))
    length = rows.shape[0]
    result = shift[None, :] + padded[0:length] * taps[0]
    result = result + padded[1:length + 1] * taps[1]
    return result + padded[2:length + 2] * taps[2]

def reference(query_proj, key_proj, value_proj, gate_proj, log_decay, residual, out_weight, norm_gain, norm_bias, up_gate, up_value, conv_weight, conv_bias, down_weight):
    length = query_proj.shape[0]
    positions = jnp.arange(length).astype(jnp.float32)
    query_rot = rotate(query_proj.astype(jnp.float32).reshape(length, RETENTION_HEADS, DK), positions).astype(jnp.bfloat16)
    key_rot = (rotate(key_proj.astype(jnp.float32).reshape(length, RETENTION_HEADS, DK), positions) * DK ** (-0.5)).astype(jnp.bfloat16)
    block_count = length // BLOCK
    asking_segments = query_rot.reshape(block_count, BLOCK, RETENTION_HEADS, DK)
    key_blocks = key_rot.reshape(block_count, BLOCK, RETENTION_HEADS, DK)
    value_blocks = value_proj.reshape(block_count, BLOCK, RETENTION_HEADS, DV)
    log_blocks = log_decay.reshape(block_count, BLOCK, RETENTION_HEADS)

    def advance(carry_state, pieces):
        within, scaled_query, summand_term, block_decay = block_parts(*pieces)
        carried = jnp.einsum('thd,hde->the', scaled_query, rounded(carry_state), precision=lax.Precision.HIGHEST)
        return (block_decay[:, None, None] * carry_state + summand_term, within + carried)
    start_state = jnp.zeros((RETENTION_HEADS, DK, DV), jnp.float32)
    _, mixed_heads = lax.scan(advance, start_state, (asking_segments, key_blocks, value_blocks, log_blocks))
    mixed_heads = mixed_heads.reshape(length, RETENTION_HEADS, DV)
    average = mixed_heads.mean(-1, keepdims=True)
    spread = jnp.square(mixed_heads - average).mean(-1, keepdims=True)
    standardized_rows = (mixed_heads - average) * lax.rsqrt(spread + tiny_stabilizer)
    gate_heads = gate_proj.astype(jnp.float32).reshape(length, RETENTION_HEADS, DV)
    gated_rows = (jax.nn.silu(gate_heads) * standardized_rows).astype(jnp.bfloat16).reshape(length, RETENTION_HEADS * DV)
    attended = grouped_product(gated_rows, out_weight, N_TP)
    normed_rows = layer_norm(alpha_scale * residual.astype(jnp.float32) + attended, norm_gain[0], norm_bias[0]).astype(jnp.bfloat16)
    gate_up = jnp.dot(normed_rows, up_gate, preferred_element_type=jnp.float32).astype(jnp.bfloat16)
    value_up = jnp.dot(normed_rows, up_value, preferred_element_type=jnp.float32).astype(jnp.bfloat16)
    gate_conv = causal_conv(gate_up, conv_weight[0], conv_bias[0])
    value_conv = causal_conv(value_up, conv_weight[1], conv_bias[1])
    activated = (jax.nn.gelu(gate_conv) * value_conv).astype(jnp.bfloat16)
    ffn_out = grouped_product(activated, down_weight, N_TP)
    return layer_norm(alpha_scale * normed_rows.astype(jnp.float32) + ffn_out, norm_gain[1], norm_bias[1]).astype(jnp.bfloat16)
```

```python
import jax
import jax.numpy as jnp
from jax import lax
from jax.sharding import Mesh
from jax.sharding import PartitionSpec as P

BLOCK = 256
SP = ("sp_0", "sp_1")
SP_TP = ("sp_0", "sp_1", "tp")


alpha_scale = 8.0**0.25
rope_base = 10000.0
tiny_stabilizer = 1e-05


def turned_gather(arrays, axis, dims):
    turned = [jnp.moveaxis(a, dim, 0) for a, dim in zip(arrays, dims)]
    both = jnp.concatenate([t.reshape(len(t), -1) for t in turned], axis=1)
    out, at, finished = (lax.all_gather(both, axis, axis=0, tiled=True), 0, [])
    for t, dim in zip(turned, dims):
        piece = out[:, at : at + t[0].size].reshape(-1, *t.shape[1:])
        finished.append(jnp.moveaxis(piece, 0, dim))
        at += t[0].size
    return tuple(finished)


def neutral_like(x, identity):
    return jax.tree.map(
        lambda a, e: jnp.broadcast_to(jnp.asarray(e, a.dtype), a.shape), x, identity
    )


def entering(x, axes, combine, identity):
    before = start = neutral_like(x, identity)
    subtotal = x
    for axis in reversed(axes):
        length, position = (lax.axis_size(axis), lax.axis_index(axis))
        pieces = jax.tree.map(
            lambda part, kind: lax.all_gather(part.astype(kind), axis),
            subtotal,
            (jnp.bfloat16, jnp.bfloat16),
        )
        inside, subtotal = (start, start)
        for k in range(length):
            passed = k < position
            subtotal = combine(
                subtotal, jax.tree.map(lambda part, own: part[k].astype(own.dtype), pieces, x)
            )
            inside = jax.tree.map(lambda new, old: jnp.where(passed, new, old), subtotal, inside)
        before = combine(inside, before)
    return before


def passed_along(x, axis, by):
    length = lax.axis_size(axis)
    pairs = [(i, i + by) for i in range(length) if 0 <= i + by < length]
    return lax.ppermute(x, axis, pairs)


def rotate(vectors, positions):
    head_width = vectors.shape[-1]
    half_width = head_width // 2
    inverse_freq = rope_base ** (-2.0 * jnp.arange(half_width, dtype=jnp.float32) / head_width)
    angles = positions[:, None] * inverse_freq[None, :]
    cosine = jnp.cos(angles)[:, None, :]
    sine_part = jnp.sin(angles)[:, None, :]
    front = vectors[..., :half_width]
    second = vectors[..., half_width:]
    return jnp.concatenate(
        [front * cosine - second * sine_part, front * sine_part + second * cosine], axis=-1
    )


def layer_norm(values, gain, shift):
    average = values.mean(-1, keepdims=True)
    spread = jnp.square(values - average).mean(-1, keepdims=True)
    return (values - average) * lax.rsqrt(spread + tiny_stabilizer) * gain + shift


def block_parts(query_tile, lookup_piece, payload_piece, log_blk):
    cum_log = jnp.cumsum(log_blk, axis=0)
    cum_heads = cum_log.T
    log_gap = cum_heads[:, :, None] - cum_heads[:, None, :]
    offsets = jnp.arange(log_blk.shape[0])
    causal = (offsets[:, None] >= offsets[None, :])[None]
    weight = jnp.where(causal, jnp.exp(jnp.where(causal, log_gap, 0.0)), 0.0)
    score_matrix = jnp.einsum(
        "jka,ska->kjs", query_tile, lookup_piece, preferred_element_type=jnp.float32
    )
    segment_scaling = (score_matrix * weight).astype(jnp.bfloat16)
    within = jnp.einsum(
        "htm,mhe->the", segment_scaling, payload_piece, preferred_element_type=jnp.float32
    )
    block_total = cum_log[-1]
    to_end = jnp.exp(block_total[None, :] - cum_log)
    faded_lookup_vector = (lookup_piece.astype(jnp.float32) * to_end[:, :, None]).astype(
        jnp.bfloat16
    )
    summand_term = jnp.einsum(
        "ajo,ajd->jod", faded_lookup_vector, payload_piece, preferred_element_type=jnp.float32
    )
    scaled_query = (query_tile.astype(jnp.float32) * jnp.exp(cum_log)[:, :, None]).astype(
        jnp.bfloat16
    )
    return (within, scaled_query, summand_term, jnp.exp(block_total))


def causal_conv(rows, edge_rows, taps, shift):
    padded = jnp.concatenate([edge_rows, rows], axis=0).astype(jnp.float32)
    length = rows.shape[0]
    result = shift[None, :] + padded[0:length] * taps[0]
    result = result + padded[1 : length + 1] * taps[1]
    return result + padded[2 : length + 2] * taps[2]


def combine(earlier, later):
    return (earlier[0] * later[0], later[0][:, None, None] * earlier[1] + later[1])


def shards(
    query_proj,
    key_proj,
    value_proj,
    gate_proj,
    log_decay,
    residual,
    out_weight,
    norm_gain,
    norm_bias,
    up_gate,
    up_value,
    conv_weight,
    conv_bias,
    down_weight,
):
    tok_rows = query_proj.shape[0]
    head_count = log_decay.shape[1]
    key_width = query_proj.shape[1] // head_count
    value_width = value_proj.shape[1] // head_count
    full_gate, full_value, full_down = turned_gather(
        (up_gate, up_value, down_weight), SP, (0, 0, 1)
    )
    positions = (lax.axis_index(SP) * tok_rows + jnp.arange(tok_rows)).astype(jnp.float32)
    query_rot = rotate(
        query_proj.astype(jnp.float32).reshape(tok_rows, head_count, key_width), positions
    ).astype(jnp.bfloat16)
    key_rot = (
        rotate(key_proj.astype(jnp.float32).reshape(tok_rows, head_count, key_width), positions)
        * key_width ** (-0.5)
    ).astype(jnp.bfloat16)
    block_count = tok_rows // BLOCK
    asking_segments = query_rot.reshape(block_count, BLOCK, head_count, key_width)
    key_blocks = key_rot.reshape(block_count, BLOCK, head_count, key_width)
    value_blocks = value_proj.reshape(block_count, BLOCK, head_count, value_width)
    log_blocks = log_decay.reshape(block_count, BLOCK, head_count)
    within, scaled_query, summand_term, block_decay = jax.vmap(block_parts)(
        asking_segments, key_blocks, value_blocks, log_blocks
    )

    def absorb(carry_state, pieces):
        return (pieces[1][:, None, None] * carry_state + pieces[0], None)

    zero_state = jnp.zeros((head_count, key_width, value_width), jnp.float32)
    own_state, _ = lax.scan(absorb, zero_state, (summand_term, block_decay))
    own_decay = jnp.prod(block_decay, axis=0)
    _, incoming = entering(
        (own_decay, own_state), SP, combine, (jnp.ones_like(own_decay), zero_state)
    )

    def advance(carry_state, pieces):
        carried = jnp.einsum(
            "thd,hde->the",
            pieces[0],
            carry_state.astype(jnp.bfloat16),
            preferred_element_type=jnp.float32,
        )
        return (pieces[2][:, None, None] * carry_state + pieces[1], carried)

    _, carried = lax.scan(advance, incoming, (scaled_query, summand_term, block_decay))
    mixed_heads = (within + carried).reshape(tok_rows, head_count, value_width)
    average = mixed_heads.mean(-1, keepdims=True)
    spread = jnp.square(mixed_heads - average).mean(-1, keepdims=True)
    standardized_rows = (mixed_heads - average) * lax.rsqrt(spread + tiny_stabilizer)
    gate_heads = gate_proj.astype(jnp.float32).reshape(tok_rows, head_count, value_width)
    gated_rows = (
        (jax.nn.silu(gate_heads) * standardized_rows)
        .astype(jnp.bfloat16)
        .reshape(tok_rows, head_count * value_width)
    )
    own_count = tok_rows // lax.axis_size("tp")
    partial_rows = jnp.dot(gated_rows, out_weight, preferred_element_type=jnp.float32)
    attended = lax.psum_scatter(
        partial_rows.astype(jnp.bfloat16), "tp", scatter_dimension=0, tiled=True
    ).astype(jnp.float32)
    own_residual = lax.dynamic_slice_in_dim(
        residual, lax.axis_index("tp") * own_count, own_count, 0
    )
    normed_own = layer_norm(
        alpha_scale * own_residual.astype(jnp.float32) + attended, norm_gain[0], norm_bias[0]
    ).astype(jnp.bfloat16)
    whole_rows = lax.all_gather(normed_own, "tp", axis=0, tiled=True)
    gate_up = jnp.dot(whole_rows, full_gate, preferred_element_type=jnp.float32)
    value_up = jnp.dot(whole_rows, full_value, preferred_element_type=jnp.float32)
    gate_up = gate_up.astype(jnp.bfloat16)
    value_up = value_up.astype(jnp.bfloat16)
    edges = jnp.concatenate([gate_up[tok_rows - 2 :], value_up[tok_rows - 2 :]], axis=0)
    edges = passed_along(edges, SP, 1)
    gate_edge, value_edge = edges[:2], edges[2:]
    gate_conv = causal_conv(gate_up, gate_edge, conv_weight[0], conv_bias[0])
    value_conv = causal_conv(value_up, value_edge, conv_weight[1], conv_bias[1])
    activated = (jax.nn.gelu(gate_conv) * value_conv).astype(jnp.bfloat16)
    partial_ffn = jnp.dot(activated, full_down, preferred_element_type=jnp.float32)
    ffn_out = lax.psum_scatter(
        partial_ffn.astype(jnp.bfloat16), "tp", scatter_dimension=0, tiled=True
    ).astype(jnp.float32)
    return layer_norm(
        alpha_scale * normed_own.astype(jnp.float32) + ffn_out, norm_gain[1], norm_bias[1]
    ).astype(jnp.bfloat16)


def solution(mesh):
    torus = Mesh(mesh.devices.reshape(4, 4, mesh.shape["tp"]), ("sp_0", "sp_1", "tp"))
    return jax.shard_map(
        shards,
        mesh=torus,
        in_specs=(
            P(SP, "tp"),
            P(SP, "tp"),
            P(SP, "tp"),
            P(SP, "tp"),
            P(SP, "tp"),
            P(SP, None),
            P("tp", None),
            P(),
            P(),
            P(SP, "tp"),
            P(SP, "tp"),
            P(None, None, "tp"),
            P(None, "tp"),
            P("tp", SP),
        ),
        out_specs=P(SP_TP, None),
        check_vma=False,
    )
```

```python
import functools

import jax
import jax.numpy as jnp
import numpy as np
from jax import lax
from jax.experimental import pallas as pl
from jax.experimental.pallas import tpu as pltpu
from jax.sharding import Mesh
from jax.sharding import PartitionSpec as P

BLOCK = 256
CHUNKS = 2
SP = ("z", "y")
TP = ("x", "c")
f32 = jnp.float32
bf16 = jnp.bfloat16

ALPHA = 8.0**0.25
ROPE_BASE = 10000.0
EPS = 1e-05
EXTRA = 16
HIGHEST = lax.Precision.HIGHEST


def ring(shift, size=4):
    return [(i, (i + shift) % size) for i in range(size)]


def shift_by(x, axis, by):
    return lax.ppermute(x, axis, ring(by))


def swap_cores(x):
    return lax.ppermute(x, "c", [(0, 1), (1, 0)])


def params(*semantics):
    return pltpu.CompilerParams(dimension_semantics=semantics or None)


def whole(shape):
    return pl.BlockSpec(shape, lambda *_: (0,) * len(shape))


def call(kernel, grid, in_specs, out_specs, out_shape, scratch=(), flops=0, read=0):
    return pl.pallas_call(
        kernel,
        grid_spec=pltpu.PrefetchScalarGridSpec(
            num_scalar_prefetch=1,
            grid=grid,
            in_specs=in_specs,
            out_specs=out_specs,
            scratch_shapes=scratch,
        ),
        out_shape=out_shape,
        cost_estimate=pl.CostEstimate(flops=flops, transcendentals=0, bytes_accessed=read),
        compiler_params=params(*("arbitrary",) * len(grid)),
    )


def trig_tables(half, rows, count):
    freq = ROPE_BASE ** (-2.0 * np.arange(half, dtype=np.float64) / (2 * half))
    low = np.arange(rows, dtype=np.float64)[:, None] * freq[None, :]
    high = rows * np.arange(count, dtype=np.float64)[:, None] * freq[None, :]
    return [np.asarray(t, np.float32) for t in (np.cos(low), np.sin(low), np.cos(high), np.sin(high))]


def rotated(x, b, cl, sl, ch, sh):
    rows = cl.shape[0]
    parts = []
    for i in range(x.shape[0] // rows):
        at = b * (x.shape[0] // rows) + i
        hc, hs = ch[pl.ds(at, 1), :], sh[pl.ds(at, 1), :]
        cos = hc * cl[...] - hs * sl[...]
        sin = hs * cl[...] + hc * sl[...]
        half = cl.shape[1]
        front = x[i * rows : (i + 1) * rows, :half]
        second = x[i * rows : (i + 1) * rows, half:]
        parts.append(
            jnp.concatenate([front * cos - second * sin, front * sin + second * cos], axis=1)
        )
    return jnp.concatenate(parts, axis=0)


def triangle(n):
    r = lax.broadcasted_iota(jnp.int32, (n, n), 0)
    c = lax.broadcasted_iota(jnp.int32, (n, n), 1)
    return r >= c


def running_logs(row, lower):
    n = lower.shape[0]
    rows = jnp.broadcast_to(row, (8, n))
    tri = lower.astype(f32)
    down = lax.dot_general(tri, rows, (((1,), (1,)), ((), ())), precision=HIGHEST, preferred_element_type=f32)
    across = lax.dot_general(rows, tri, (((1,), (1,)), ((), ())), precision=HIGHEST, preferred_element_type=f32)
    return down[:, 0:1], across[0:1, :]


def log_rows(total, width):
    a = total.astype(bf16)
    b = (total - a.astype(f32)).astype(bf16)
    c = (total - a.astype(f32) - b.astype(f32)).astype(bf16)
    at = lax.broadcasted_iota(jnp.int32, (EXTRA, width), 0)
    pick = jnp.where(at == 0, a.astype(f32), jnp.where(at == 1, b.astype(f32), c.astype(f32)))
    return jnp.where(at < 3, pick, 0.0).astype(bf16)


def log_of(rows):
    return rows[0:1, 0:1] + rows[1:2, 0:1] + rows[2:3, 0:1]


def states_kernel(sc, log, k, v, cl, sl, ch, sh, kr, prefix, p0, p1, p2, p3, state):
    b = pl.program_id(0)
    lower = triangle(BLOCK)
    cum, _ = running_logs(log[pl.ds(b, 1), :], lower)
    total = cum[BLOCK - 1 : BLOCK, :]
    key = (rotated(k[...].astype(f32), b, cl, sl, ch, sh) * k.shape[1] ** (-0.5)).astype(bf16)
    kr[...] = key
    faded = (key.astype(f32) * jnp.exp(total - cum)).astype(bf16)
    add = lax.dot_general(faded, v[...], (((0,), (0,)), ((), ())), preferred_element_type=f32)

    @pl.when(b == 0)
    def _():
        state[...] = jnp.zeros_like(state)

    prefix[0] = state[...].astype(bf16)
    state[...] = jnp.exp(total) * state[...] + add

    @pl.when(b == pl.num_programs(0) - 1)
    def _():
        everything = jnp.sum(jnp.sum(log[...], axis=1, keepdims=True), axis=0, keepdims=True)
        tail = log_rows(everything, state.shape[1])
        rows = state.shape[0] // 4
        for d, out in enumerate((p0, p1, p2, p3)):
            at = pl.multiple_of(lax.rem(sc[1] + d, 4) * rows, rows)
            out[:rows] = state[pl.ds(at, rows), :].astype(bf16)
            out[rows:] = tail


def line_kernel(sc, r0, r1, r2, r3, total, entry, logs, pieces):
    rows = entry.shape[1]
    for d, r in enumerate((r0, r1, r2, r3)):
        pieces[lax.rem(sc[1] + 4 - d, 4)] = r[...]
    run = jnp.zeros(entry.shape[1:], f32)
    passed = jnp.zeros((1, 1), f32)
    for j in range(4):
        entry[j] = run
        logs[j : j + 1, :] = jnp.broadcast_to(passed, (1, logs.shape[1]))
        here = log_of(pieces[j, rows:].astype(f32))
        run = jnp.exp(here) * run + pieces[j, :rows].astype(f32)
        passed = passed + here
    total[:rows] = run.astype(bf16)
    total[rows:] = log_rows(passed, total.shape[1])


def incoming_kernel(sc, t1, t2, t3, entry, logs, o0, o1, o2, o3):
    rows = entry.shape[1]
    run = jnp.zeros(entry.shape[1:], f32)
    for d, t in ((3, t3), (2, t2), (1, t1)):
        new = jnp.exp(log_of(t[rows:].astype(f32))) * run + t[:rows].astype(f32)
        run = jnp.where(sc[0] >= d, new, run)
    for d, out in enumerate((o0, o1, o2, o3)):
        at = lax.rem(sc[1] + d, 4)
        fade = jnp.exp(logs[pl.ds(at, 1), 0:1])
        out[...] = (fade * run + entry[at]).astype(bf16)


def regroup(rows):
    n = rows.shape[0] // 4
    return [jnp.concatenate([rows[i * n : (i + 1) * n], rows[(i + 2) * n : (i + 3) * n]], axis=0) for i in range(2)]


def within_kernel(sc, log, q, kr, v, cl, sl, ch, sh, within, scaled):
    b = pl.program_id(0)
    lower = triangle(BLOCK)
    cum, across = running_logs(log[pl.ds(b, 1), :], lower)
    query = rotated(q[...].astype(f32), b, cl, sl, ch, sh).astype(bf16)
    score = lax.dot_general(query, kr[...], (((1,), (1,)), ((), ())), preferred_element_type=f32)
    weight = jnp.where(lower, jnp.exp(jnp.where(lower, cum - across, 0.0)), 0.0)
    result = jnp.dot((score * weight).astype(bf16), v[...], preferred_element_type=f32)
    faded = (query.astype(f32) * jnp.exp(cum)).astype(bf16)
    for i, (w, s) in enumerate(zip(regroup(result), regroup(faded))):
        within[i, 0] = w
        scaled[i, 0] = s


def heads_kernel(sc, log, i0, i1, i2, i3, prefix, within, scaled, gate, weight, keep, send, start):
    b = pl.program_id(0)
    rows = i0.shape[0]

    @pl.when(b == 0)
    def _():
        for d, piece in enumerate((i0, i1, i2, i3)):
            at = pl.multiple_of(lax.rem(sc[1] + 4 - d, 4) * rows, rows)
            start[pl.ds(at, rows), :] = piece[...].astype(f32)

    per_block = jnp.sum(log[...], axis=1, keepdims=True)
    earlier = lax.broadcasted_iota(jnp.int32, per_block.shape, 0) < b
    passed = jnp.sum(jnp.where(earlier, per_block, 0.0), axis=0, keepdims=True)
    state = (jnp.exp(passed) * start[...] + prefix[0].astype(f32)).astype(bf16)
    mixed = within[0, 0] + jnp.dot(scaled[0, 0], state, preferred_element_type=f32)
    centred = mixed - jnp.mean(mixed, axis=1, keepdims=True)
    spread = jnp.mean(centred * centred, axis=1, keepdims=True)
    g = gate[...].astype(f32).reshape(mixed.shape)
    gated = (g * jax.nn.sigmoid(g) * (centred * lax.rsqrt(spread + EPS))).astype(bf16)
    part = jnp.dot(gated, weight[...], preferred_element_type=f32).astype(bf16)
    n = part.shape[0] // 2
    south = sc[3] == 0
    keep[0] = jnp.where(south, part[:n], part[n:])
    send[0] = jnp.where(south, part[n:], part[:n])


def both(keep, got, d, cols):
    return keep[d, :, cols].astype(f32) + got[d, :, cols].astype(f32)


def halves(width):
    return slice(0, width // 2), slice(width // 2, width)


def scatter_first_kernel(sc, keep, got, up, down):
    a, b = halves(up.shape[1])
    up[:, a] = both(keep, got, 2, a).astype(bf16)
    up[:, b] = both(keep, got, 1, b).astype(bf16)
    down[:, a] = both(keep, got, 3, a).astype(bf16)
    down[:, b] = both(keep, got, 2, b).astype(bf16)


def scatter_second_kernel(sc, keep, got, from_below, from_above, up, down):
    a, b = halves(from_below.shape[1])
    up[...] = (both(keep, got, 1, a) + from_below[:, a].astype(f32)).astype(bf16)
    down[...] = (both(keep, got, 3, b) + from_above[:, b].astype(f32)).astype(bf16)


def scatter_norm_kernel(sc, keep, got, from_below, from_above, far_a, far_b, base, gain, shift, out, row):
    width = out.shape[1]
    a, b = halves(width)
    left = both(keep, got, 0, a) + from_above[:, a].astype(f32) + far_a[...].astype(f32)
    right = both(keep, got, 0, b) + from_below[:, b].astype(f32) + far_b[...].astype(f32)
    total = jnp.concatenate([left, right], axis=1) + ALPHA * base[0].astype(f32)
    centred = total - jnp.mean(total, axis=1, keepdims=True)
    spread = jnp.mean(centred * centred, axis=1, keepdims=True)
    out[...] = (
        centred * lax.rsqrt(spread + EPS) * gain[row : row + 1, :] + shift[row : row + 1, :]
    ).astype(bf16)


def reduce_and_norm(sc, keep, send, base, base_index, gain, shift, row):
    _, rows, width = keep.shape
    piece = jax.ShapeDtypeStruct((rows, width), bf16)
    half = jax.ShapeDtypeStruct((rows, width // 2), bf16)
    got = swap_cores(send)
    size = rows * width
    up, down = call(
        scatter_first_kernel, (1,), [whole(keep.shape)] * 2, [whole(piece.shape)] * 2, [piece] * 2,
        flops=size * 4, read=size * 24,
    )(sc, keep, got)
    from_below, from_above = shift_by(up, "x", 1), shift_by(down, "x", 3)
    up, down = call(
        scatter_second_kernel, (1,), [whole(keep.shape)] * 2 + [whole(piece.shape)] * 2,
        [whole(half.shape)] * 2, [half] * 2, flops=size * 4, read=size * 24,
    )(sc, keep, got, from_below, from_above)
    far_a, far_b = shift_by(up, "x", 1), shift_by(down, "x", 3)
    return call(
        functools.partial(scatter_norm_kernel, row=row),
        (1,),
        [whole(keep.shape)] * 2 + [whole(piece.shape)] * 2 + [whole(half.shape)] * 2
        + [pl.BlockSpec((1, rows, width), base_index), whole(gain.shape), whole(shift.shape)],
        whole(piece.shape),
        piece,
        flops=size * 16, read=size * 24,
    )(sc, keep, got, from_below, from_above, far_a, far_b, base, gain, shift)


def gather_rows(own):
    width = own.shape[1]
    a, b = halves(width)
    below, above = shift_by(own, "x", 1), shift_by(own, "x", 3)
    far_a, far_b = shift_by(below[:, a], "x", 1), shift_by(above[:, b], "x", 3)
    mine = [own, below, above, far_a, far_b]
    return mine + [swap_cores(m) for m in mine]


def up_kernel(sc, *refs):
    pieces, weight, out, rows, total = refs[:10], refs[10], refs[11], refs[12], refs[13]
    step = pl.program_id(0)
    n, width = pieces[0].shape
    a, b = halves(width)

    @pl.when(step == 0)
    def _():
        for side in range(2):
            core = sc[3] if side == 0 else 1 - sc[3]
            own, below, above, far_a, far_b = pieces[5 * side : 5 * side + 5]
            for d, r in ((0, own), (3, below), (1, above)):
                at = pl.multiple_of((2 * lax.rem(sc[2] + d, 4) + core) * n, n)
                rows[pl.ds(at, n), :] = r[...]
            at = pl.multiple_of((2 * lax.rem(sc[2] + 2, 4) + core) * n, n)
            rows[pl.ds(at, n), a] = far_a[...]
            rows[pl.ds(at, n), b] = far_b[...]

    deep = weight.shape[0]
    left = rows[:, pl.ds(pl.multiple_of(step * deep, deep), deep)]
    part = jnp.dot(left, weight[...], preferred_element_type=f32)

    @pl.when(step == 0)
    def _():
        total[...] = part

    @pl.when(step > 0)
    def _():
        total[...] += part

    @pl.when(step == pl.num_programs(0) - 1)
    def _():
        out[...] = total[...].astype(bf16)


def up_project(sc, pieces, weights, hidden):
    n, width = pieces[0].shape
    steps = 4
    rows = 8 * n
    return call(
        up_kernel,
        (steps,),
        [whole(p.shape) for p in pieces] + [pl.BlockSpec((width // steps, hidden), lambda i, s: (i, 0))],
        whole((rows, hidden)),
        jax.ShapeDtypeStruct((rows, hidden), bf16),
        scratch=[pltpu.VMEM((rows, width), bf16), pltpu.VMEM((rows, hidden), f32)],
        flops=2 * rows * width * hidden, read=2 * width * hidden + 4 * rows * width,
    )(sc, *pieces, weights)


def down_kernel(sc, mine, other, edge, taps, bias, weight, keep, send, active, padded, chunk):
    step = pl.program_id(0)
    n = keep.shape[1]
    hidden = active.shape[1]

    @pl.when(step == 0)
    def _():
        for t in range(8):
            if chunk == 1:
                halo = other[t * n + n - 8 : t * n + n, :]
            elif t > 0:
                halo = other[t * n - 8 : t * n, :]
            else:
                halo = edge[...]
            padded[0:8] = halo.astype(f32)
            padded[8:] = mine[t * n : (t + 1) * n, :].astype(f32)
            conv = bias[0:1, :] + padded[6 : 6 + n] * taps[0:1, :]
            conv = conv + padded[7 : 7 + n] * taps[1:2, :]
            conv = conv + padded[8 : 8 + n] * taps[2:3, :]
            active[t * n : (t + 1) * n, :] = (
                jax.nn.gelu(conv[:, :hidden]) * conv[:, hidden:]
            ).astype(bf16)

    part = lax.dot_general(
        active[...], weight[:, :hidden], (((1,), (1,)), ((), ())), preferred_element_type=f32
    ).astype(bf16)
    south = sc[3] == 0
    for xx in range(4):
        lo, hi = part[2 * xx * n : (2 * xx + 1) * n], part[(2 * xx + 1) * n : (2 * xx + 2) * n]
        at = lax.rem(xx + 4 - sc[2], 4)
        keep[at] = jnp.where(south, lo, hi)
        send[at] = jnp.where(south, hi, lo)


def down_project(sc, mine, other, edge, taps, bias, weights, width, chunk):
    rows, double = mine.shape
    hidden = double // 2
    n = rows // 8
    steps = 4
    cols = width // steps
    shape = jax.ShapeDtypeStruct((4, n, width), bf16)
    out = pl.BlockSpec((4, n, cols), lambda i, s: (0, 0, i))
    return call(
        functools.partial(down_kernel, chunk=chunk),
        (steps,),
        [whole(mine.shape), whole(other.shape), whole(edge.shape), whole(taps.shape), whole(bias.shape),
         pl.BlockSpec((cols, double), lambda i, s: (i, 1))],
        [out, out],
        [shape, shape],
        scratch=[pltpu.VMEM((rows, hidden), bf16), pltpu.VMEM((n + 8, double), f32)],
        flops=2 * rows * width * hidden, read=2 * width * hidden + 4 * rows * width,
    )(sc, mine, other, edge, taps, bias, weights)


def shards(
    query_proj, key_proj, value_proj, gate_proj, log_decay, residual, out_weight, norm_gain,
    norm_bias, up_gate, up_value, conv_weight, conv_bias, down_weight,
):
    tok, dk = query_proj.shape
    dv = value_proj.shape[1]
    width = residual.shape[1]
    hidden = up_gate.shape[1]
    blocks = tok // BLOCK
    n = tok // 16
    shard = jnp.concatenate([up_gate, up_value, down_weight.T], axis=1)
    weights = lax.all_gather(shard, SP, axis=0, tiled=True)
    taps = jnp.concatenate([conv_weight[0], conv_weight[1]], axis=1)
    bias = jnp.concatenate([conv_bias[0:1], conv_bias[1:2]], axis=1)
    sc = jnp.stack([lax.axis_index(a) for a in ("z", "y", "x", "c")]).astype(jnp.int32)

    log = log_decay.reshape(blocks, BLOCK)
    cl, sl, ch, sh = trig_tables(dk // 2, 128, 16 * tok // 128)
    high = pl.BlockSpec((tok // 128, dk // 2), lambda i, s: (4 * s[0] + s[1], 0))
    tables = [whole(cl.shape), whole(sl.shape), high, high]
    by_block = lambda w: pl.BlockSpec((BLOCK, w), lambda i, s: (i, 0))
    piece = jax.ShapeDtypeStruct((dk // 4 + EXTRA, dv), bf16)
    key_rot, prefix, *pieces = call(
        states_kernel,
        (blocks,),
        [whole(log.shape), by_block(dk), by_block(dv)] + tables,
        [by_block(dk), pl.BlockSpec((1, dk, dv), lambda i, s: (i, 0, 0))] + [whole(piece.shape)] * 4,
        [jax.ShapeDtypeStruct((tok, dk), bf16), jax.ShapeDtypeStruct((blocks, dk, dv), bf16)] + [piece] * 4,
        scratch=[pltpu.VMEM((dk, dv), f32)],
        flops=4 * tok * dk * dv, read=6 * tok * dv,
    )(sc, log, key_proj, value_proj, cl, sl, ch, sh)
    got = [pieces[0]] + [shift_by(pieces[d], "y", d) for d in (1, 2, 3)]
    entry = jax.ShapeDtypeStruct((4, dk // 4, dv), f32)
    logs = jax.ShapeDtypeStruct((8, 128), f32)
    total, entry, logs = call(
        line_kernel,
        (1,),
        [whole(piece.shape)] * 4,
        [whole(piece.shape), whole(entry.shape), whole(logs.shape)],
        [piece, entry, logs],
        scratch=[pltpu.VMEM((4,) + piece.shape, bf16)],
        flops=10 * dk * dv, read=8 * dk * dv,
    )(sc, *got)
    lines = [shift_by(total, "z", d) for d in (1, 2, 3)]
    quarter = jax.ShapeDtypeStruct((dk // 4, dv), bf16)
    outgoing = call(
        incoming_kernel,
        (1,),
        [whole(piece.shape)] * 3 + [whole(entry.shape), whole(logs.shape)],
        [whole(quarter.shape)] * 4,
        [quarter] * 4,
        flops=10 * dk * dv, read=8 * dk * dv,
    )(sc, *lines, entry, logs)
    incoming = [outgoing[0]] + [shift_by(outgoing[d], "y", d) for d in (1, 2, 3)]

    by_chunk = lambda w: pl.BlockSpec((2, 1, 2 * n, w), lambda i, s: (0, i, 0, 0))
    within, scaled = call(
        within_kernel,
        (blocks,),
        [whole(log.shape), by_block(dk), by_block(dk), by_block(dv)] + tables,
        [by_chunk(dv), by_chunk(dk)],
        [jax.ShapeDtypeStruct((2, blocks, 2 * n, dv), f32), jax.ShapeDtypeStruct((2, blocks, 2 * n, dk), bf16)],
        flops=4 * tok * BLOCK * (dk + dv), read=8 * tok * dv,
    )(sc, log, query_proj, key_rot, value_proj, cl, sl, ch, sh)

    gates = gate_proj.reshape(blocks, 2, 2, n, dv)
    bases = residual.reshape(16, n, width)
    normed, ups = [None, None], [None, None]
    for k in (1, 0):
        one = lambda w, k=k: pl.BlockSpec((1, 1, 2 * n, w), lambda i, s: (k, i, 0, 0))
        lane = pl.BlockSpec((1, n, width), lambda i, s: (lax.rem(i + 4 - s[2], 4), 0, 0))
        shape = jax.ShapeDtypeStruct((4, n, width), bf16)
        keep, send = call(
            heads_kernel,
            (blocks,),
            [whole(log.shape)] + [whole(quarter.shape)] * 4
            + [pl.BlockSpec((1, dk, dv), lambda i, s: (i, 0, 0)), one(dv), one(dk),
               pl.BlockSpec((1, 2, 1, n, dv), lambda i, s, k=k: (i, 0, k, 0, 0)), whole(out_weight.shape)],
            [lane, lane],
            [shape, shape],
            scratch=[pltpu.VMEM((dk, dv), f32)],
            flops=tok * dv * (dk + width), read=8 * tok * dv,
        )(sc, log, *incoming, prefix, within, scaled, gates, out_weight)
        normed[k] = reduce_and_norm(
            sc, keep, send, bases, lambda i, s, k=k: (4 * s[2] + 2 * s[3] + k, 0, 0), norm_gain, norm_bias, 0
        )
    for k in (1, 0):
        ups[k] = up_project(sc, gather_rows(normed[k]), weights, 2 * hidden)
    last = ups[1][8 * n - 8 :]
    edge = lax.ppermute(last, SP, [(i, i + 1) for i in range(15)])
    outs = []
    for k in (0, 1):
        keep, send = down_project(sc, ups[k], ups[1 - k], edge, taps, bias, weights, width, k)
        outs.append(
            reduce_and_norm(sc, keep, send, normed[k][None], lambda i, s: (0, 0, 0), norm_gain, norm_bias, 1)
        )
    return jnp.concatenate(outs, axis=0)


def solution(mesh):
    torus = Mesh(mesh.devices.reshape(4, 4, 4, 2), SP + TP)
    return jax.shard_map(
        shards,
        mesh=torus,
        in_specs=(
            P(SP, TP),
            P(SP, TP),
            P(SP, TP),
            P(SP, TP),
            P(SP, TP),
            P(SP, None),
            P(TP, None),
            P(),
            P(),
            P(SP, TP),
            P(SP, TP),
            P(None, None, TP),
            P(None, TP),
            P(TP, SP),
        ),
        out_specs=P(SP + TP, None),
        check_vma=False,
    )
```

```python
import functools

import jax
import jax.numpy as jnp
import numpy as np
from jax import lax
from jax.experimental import pallas as pl
from jax.experimental.pallas import tpu as pltpu
from jax.sharding import Mesh
from jax.sharding import PartitionSpec as P

BLOCK = 256
CHUNKS = 2
SP = ("z", "y")
TP = ("x", "c")
f32 = jnp.float32
bf16 = jnp.bfloat16

ALPHA = 8.0**0.25
ROPE_BASE = 10000.0
EPS = 1e-05
EXTRA = 16
HIGHEST = lax.Precision.HIGHEST


def ring(shift, size=4):
    return [(i, (i + shift) % size) for i in range(size)]


def shift_by(x, axis, by):
    return lax.ppermute(x, axis, ring(by))


def swap_cores(x):
    return lax.ppermute(x, "c", [(0, 1), (1, 0)])


def call(kernel, sc, args, outs, scratch=(), flops=0, limit=8):
    near = pl.BlockSpec(memory_space=pltpu.VMEM)
    return pl.pallas_call(
        kernel,
        in_specs=[pl.BlockSpec(memory_space=pltpu.SMEM)] + [near] * len(args),
        out_specs=[near] * len(outs),
        out_shape=[pltpu.VMEM(shape, dtype) for shape, dtype in outs],
        scratch_shapes=scratch,
        cost_estimate=pl.CostEstimate(flops=flops, transcendentals=0, bytes_accessed=0),
        compiler_params=pltpu.CompilerParams(vmem_limit_bytes=limit << 20),
    )(sc, *[pltpu.with_memory_space_constraint(a, pltpu.VMEM) for a in args])


def trig_tables(half, rows, count):
    freq = ROPE_BASE ** (-2.0 * np.arange(half, dtype=np.float64) / (2 * half))
    low = np.arange(rows, dtype=np.float64)[:, None] * freq[None, :]
    high = rows * np.arange(count, dtype=np.float64)[:, None] * freq[None, :]
    return [np.asarray(t, np.float32) for t in (np.cos(low), np.sin(low), np.cos(high), np.sin(high))]


def rotated(x, b, cl, sl, ch, sh):
    rows = cl.shape[0]
    parts = []
    for i in range(x.shape[0] // rows):
        at = b * (x.shape[0] // rows) + i
        hc, hs = ch[pl.ds(at, 1), :], sh[pl.ds(at, 1), :]
        cos = hc * cl[...] - hs * sl[...]
        sin = hs * cl[...] + hc * sl[...]
        half = cl.shape[1]
        front = x[i * rows : (i + 1) * rows, :half]
        second = x[i * rows : (i + 1) * rows, half:]
        parts.append(
            jnp.concatenate([front * cos - second * sin, front * sin + second * cos], axis=1)
        )
    return jnp.concatenate(parts, axis=0)


def triangle(n):
    r = lax.broadcasted_iota(jnp.int32, (n, n), 0)
    c = lax.broadcasted_iota(jnp.int32, (n, n), 1)
    return r >= c


def running_logs(row, lower):
    n = lower.shape[0]
    rows = jnp.broadcast_to(row, (8, n))
    tri = lower.astype(f32)
    down = lax.dot_general(tri, rows, (((1,), (1,)), ((), ())), precision=HIGHEST, preferred_element_type=f32)
    across = lax.dot_general(rows, tri, (((1,), (1,)), ((), ())), precision=HIGHEST, preferred_element_type=f32)
    return down[:, 0:1], across[0:1, :]


def log_rows(total, width):
    a = total.astype(bf16)
    b = (total - a.astype(f32)).astype(bf16)
    c = (total - a.astype(f32) - b.astype(f32)).astype(bf16)
    at = lax.broadcasted_iota(jnp.int32, (EXTRA, width), 0)
    pick = jnp.where(at == 0, a.astype(f32), jnp.where(at == 1, b.astype(f32), c.astype(f32)))
    return jnp.where(at < 3, pick, 0.0).astype(bf16)


def log_of(rows):
    return rows[0:1, 0:1] + rows[1:2, 0:1] + rows[2:3, 0:1]


def states_kernel(sc, log, k, v, cl, sl, ch, sh, kr, prefix, p0, p1, p2, p3, state):
    lower = triangle(BLOCK)
    state[...] = jnp.zeros_like(state)

    def step(b, _):
        at = pl.ds(pl.multiple_of(b * BLOCK, BLOCK), BLOCK)
        cum, _ = running_logs(log[pl.ds(b, 1), :], lower)
        total = cum[BLOCK - 1 : BLOCK, :]
        key = rotated(k[at, :].astype(f32), b, cl, sl, ch, sh) * k.shape[1] ** (-0.5)
        key = key.astype(bf16)
        kr[at, :] = key
        faded = (key.astype(f32) * jnp.exp(total - cum)).astype(bf16)
        add = lax.dot_general(faded, v[at, :], (((0,), (0,)), ((), ())), preferred_element_type=f32)
        prefix[b] = state[...].astype(bf16)
        state[...] = jnp.exp(total) * state[...] + add
        return 0

    lax.fori_loop(0, log.shape[0], step, 0)
    everything = jnp.sum(jnp.sum(log[...], axis=1, keepdims=True), axis=0, keepdims=True)
    tail = log_rows(everything, state.shape[1])
    rows = state.shape[0] // 4
    for d, out in enumerate((p0, p1, p2, p3)):
        at = pl.multiple_of(lax.rem(sc[1] + d, 4) * rows, rows)
        out[:rows] = state[pl.ds(at, rows), :].astype(bf16)
        out[rows:] = tail


def line_kernel(sc, r0, r1, r2, r3, total, entry, logs, pieces):
    rows = entry.shape[1]
    for d, r in enumerate((r0, r1, r2, r3)):
        pieces[lax.rem(sc[1] + 4 - d, 4)] = r[...]
    run = jnp.zeros(entry.shape[1:], f32)
    passed = jnp.zeros((1, 1), f32)
    for j in range(4):
        entry[j] = run
        logs[j : j + 1, :] = jnp.broadcast_to(passed, (1, logs.shape[1]))
        here = log_of(pieces[j, rows:].astype(f32))
        run = jnp.exp(here) * run + pieces[j, :rows].astype(f32)
        passed = passed + here
    total[:rows] = run.astype(bf16)
    total[rows:] = log_rows(passed, total.shape[1])


def incoming_kernel(sc, t1, t2, t3, entry, logs, o0, o1, o2, o3):
    rows = entry.shape[1]
    run = jnp.zeros(entry.shape[1:], f32)
    for d, t in ((3, t3), (2, t2), (1, t1)):
        new = jnp.exp(log_of(t[rows:].astype(f32))) * run + t[:rows].astype(f32)
        run = jnp.where(sc[0] >= d, new, run)
    for d, out in enumerate((o0, o1, o2, o3)):
        at = lax.rem(sc[1] + d, 4)
        fade = jnp.exp(logs[pl.ds(at, 1), 0:1])
        out[...] = (fade * run + entry[at]).astype(bf16)


def within_kernel(sc, log, q, kr, v, cl, sl, ch, sh, within, scaled):
    lower = triangle(BLOCK)
    n = BLOCK // 4

    def step(b, _):
        at = pl.ds(pl.multiple_of(b * BLOCK, BLOCK), BLOCK)
        cum, across = running_logs(log[pl.ds(b, 1), :], lower)
        query = rotated(q[at, :].astype(f32), b, cl, sl, ch, sh).astype(bf16)
        score = lax.dot_general(query, kr[at, :], (((1,), (1,)), ((), ())), preferred_element_type=f32)
        weight = jnp.where(lower, jnp.exp(jnp.where(lower, cum - across, 0.0)), 0.0)
        result = jnp.dot((score * weight).astype(bf16), v[at, :], preferred_element_type=f32)
        faded = (query.astype(f32) * jnp.exp(cum)).astype(bf16)
        for i in range(4):
            within[i % 2, b, (i // 2) * n : (i // 2 + 1) * n] = result[i * n : (i + 1) * n]
            scaled[i % 2, b, (i // 2) * n : (i // 2 + 1) * n] = faded[i * n : (i + 1) * n]
        return 0

    lax.fori_loop(0, log.shape[0], step, 0)


def heads_kernel(sc, log, i0, i1, i2, i3, prefix, within, scaled, gate, weight, keep, send, start, chunk):
    rows = i0.shape[0]
    for d, piece in enumerate((i0, i1, i2, i3)):
        at = pl.multiple_of(lax.rem(sc[1] + 4 - d, 4) * rows, rows)
        start[pl.ds(at, rows), :] = piece[...].astype(f32)
    per_block = jnp.sum(log[...], axis=1, keepdims=True)
    order = lax.broadcasted_iota(jnp.int32, per_block.shape, 0)
    n = keep.shape[1]
    south = sc[3] == 0

    def step(b, _):
        passed = jnp.sum(jnp.where(order < b, per_block, 0.0), axis=0, keepdims=True)
        state = (jnp.exp(passed) * start[...] + prefix[b].astype(f32)).astype(bf16)
        mixed = within[chunk, b] + jnp.dot(scaled[chunk, b], state, preferred_element_type=f32)
        centred = mixed - jnp.mean(mixed, axis=1, keepdims=True)
        spread = jnp.mean(centred * centred, axis=1, keepdims=True)
        g = jnp.concatenate([gate[2 * b, chunk], gate[2 * b + 1, chunk]], axis=0).astype(f32)
        gated = (g * jax.nn.sigmoid(g) * (centred * lax.rsqrt(spread + EPS))).astype(bf16)
        part = jnp.dot(gated, weight[...], preferred_element_type=f32).astype(bf16)
        at = lax.rem(b + 4 - sc[2], 4)
        keep[at] = jnp.where(south, part[:n], part[n:])
        send[at] = jnp.where(south, part[n:], part[:n])
        return 0

    lax.fori_loop(0, log.shape[0], step, 0)


def scatter_kernel(sc, keep, got, s1, s2, s3):
    for d, out in ((1, s1), (2, s2), (3, s3)):
        out[...] = (keep[d].astype(f32) + got[d].astype(f32)).astype(bf16)


def norm_kernel(sc, keep, got, r1, r2, r3, base, gain, shift, out, row, group):
    total = keep[0].astype(f32) + got[0].astype(f32) + r1[...].astype(f32)
    total = total + r2[...].astype(f32) + r3[...].astype(f32)
    at = 0 if group is None else 4 * sc[2] + 2 * sc[3] + group
    total = total + ALPHA * base[at].astype(f32)
    centred = total - jnp.mean(total, axis=1, keepdims=True)
    spread = jnp.mean(centred * centred, axis=1, keepdims=True)
    out[...] = (
        centred * lax.rsqrt(spread + EPS) * gain[row : row + 1, :] + shift[row : row + 1, :]
    ).astype(bf16)


def reduce_and_norm(sc, keep, send, base, gain, shift, row, group):
    _, rows, width = keep.shape
    piece = ((rows, width), bf16)
    got = swap_cores(send)
    size = rows * width
    sums = call(scatter_kernel, sc, (keep, got), [piece] * 3, flops=size * 400)
    far = [shift_by(s, "x", d) for d, s in zip((1, 2, 3), sums)]
    return call(
        functools.partial(norm_kernel, row=row, group=group),
        sc, (keep, got, *far, base, gain, shift), [piece], flops=size * 400,
    )[0]


def gather_rows(own):
    mine = [own] + [shift_by(own, "x", d) for d in (1, 2, 3)]
    return mine + [swap_cores(m) for m in mine]


def up_kernel(sc, *refs):
    pieces, weight, out, rows = refs[:8], refs[8], refs[9], refs[10]
    n = pieces[0].shape[0]
    for i, piece in enumerate(pieces):
        core = sc[3] if i < 4 else 1 - sc[3]
        at = pl.multiple_of((2 * lax.rem(sc[2] + 4 - i % 4, 4) + core) * n, n)
        rows[pl.ds(at, n), :] = piece[...]
    out[...] = jnp.dot(rows[...], weight[:, : out.shape[1]], preferred_element_type=f32).astype(bf16)


def up_project(sc, pieces, weights, hidden):
    n, width = pieces[0].shape
    return call(
        up_kernel, sc, (*pieces, weights), [((8 * n, hidden), bf16)],
        scratch=[pltpu.VMEM((8 * n, width), bf16)], flops=16 * n * width * hidden, limit=16,
    )[0]


def down_kernel(sc, mine, other, edge, taps, bias, weight, keep, send, active, padded, chunk):
    n = keep.shape[1]
    hidden = active.shape[1]

    def conv_group(t, _):
        at = pl.multiple_of(t * n, n)
        if chunk == 1:
            halo = other[pl.ds(pl.multiple_of(at + n - 16, 16), 16), :][8:]
        else:
            before = pl.multiple_of(jnp.maximum(at - 16, 0), 16)
            halo = jnp.where(t == 0, edge[8:].astype(f32), other[pl.ds(before, 16), :][8:].astype(f32))
        padded[0:8] = halo.astype(f32)
        padded[8:] = mine[pl.ds(at, n), :].astype(f32)
        conv = bias[0:1, :] + padded[6 : 6 + n] * taps[0:1, :]
        conv = conv + padded[7 : 7 + n] * taps[1:2, :]
        conv = conv + padded[8 : 8 + n] * taps[2:3, :]
        active[pl.ds(at, n), :] = (jax.nn.gelu(conv[:, :hidden]) * conv[:, hidden:]).astype(bf16)
        return 0

    lax.fori_loop(0, 8, conv_group, 0)
    south = sc[3] == 0
    tile = 512
    for j in range(keep.shape[2] // tile):
        cols = slice(j * tile, (j + 1) * tile)
        part = lax.dot_general(
            active[...], weight[cols, 2 * hidden :], (((1,), (1,)), ((), ())), preferred_element_type=f32
        ).astype(bf16)
        for xx in range(4):
            lo, hi = part[2 * xx * n : (2 * xx + 1) * n], part[(2 * xx + 1) * n : (2 * xx + 2) * n]
            at = lax.rem(xx + 4 - sc[2], 4)
            keep[at, :, cols] = jnp.where(south, lo, hi)
            send[at, :, cols] = jnp.where(south, hi, lo)


def down_project(sc, mine, other, edge, taps, bias, weights, width, chunk):
    rows, double = mine.shape
    n = rows // 8
    shape = ((4, n, width), bf16)
    return call(
        functools.partial(down_kernel, chunk=chunk), sc,
        (mine, other, edge, taps, bias, weights), [shape, shape],
        scratch=[pltpu.VMEM((rows, double // 2), bf16), pltpu.VMEM((n + 8, double), f32)],
        flops=rows * width * double * 2, limit=16,
    )


def shards(
    query_proj, key_proj, value_proj, gate_proj, log_decay, residual, out_weight, norm_gain,
    norm_bias, up_gate, up_value, conv_weight, conv_bias, down_weight,
):
    tok, dk = query_proj.shape
    dv = value_proj.shape[1]
    width = residual.shape[1]
    hidden = up_gate.shape[1]
    blocks = tok // BLOCK
    n = tok // 16
    shard = jnp.concatenate([up_gate, up_value, down_weight.T], axis=1)
    weights = lax.all_gather(shard, SP, axis=0, tiled=True)
    taps = jnp.concatenate([conv_weight[0], conv_weight[1]], axis=1)
    bias = jnp.concatenate([conv_bias[0:1], conv_bias[1:2]], axis=1)
    sc = jnp.stack([lax.axis_index(a) for a in ("z", "y", "x", "c")]).astype(jnp.int32)

    log = log_decay.reshape(blocks, BLOCK)
    cl, sl, ch, sh = trig_tables(dk // 2, 128, 16 * tok // 128)
    ch, sh = [lax.dynamic_slice_in_dim(jnp.asarray(t), (4 * sc[0] + sc[1]) * (tok // 128), tok // 128, 0) for t in (ch, sh)]
    tables = (jnp.asarray(cl), jnp.asarray(sl), ch, sh)
    piece = ((dk // 4 + EXTRA, dv), bf16)
    key_rot, prefix, *pieces = call(
        states_kernel, sc, (log, key_proj, value_proj, *tables),
        [((tok, dk), bf16), ((blocks, dk, dv), bf16)] + [piece] * 4,
        scratch=[pltpu.VMEM((dk, dv), f32)], flops=4 * tok * dk * dv,
    )
    got = [pieces[0]] + [shift_by(pieces[d], "y", d) for d in (1, 2, 3)]
    total, entry, logs = call(
        line_kernel, sc, got, [piece, ((4, dk // 4, dv), f32), ((8, 128), f32)],
        scratch=[pltpu.VMEM((4,) + piece[0], bf16)], flops=100 * dk * dv,
    )
    lines = [shift_by(total, "z", d) for d in (1, 2, 3)]
    quarter = ((dk // 4, dv), bf16)
    outgoing = call(incoming_kernel, sc, (*lines, entry, logs), [quarter] * 4, flops=100 * dk * dv)
    incoming = [outgoing[0]] + [shift_by(outgoing[d], "y", d) for d in (1, 2, 3)]

    within, scaled = call(
        within_kernel, sc, (log, query_proj, key_rot, value_proj, *tables),
        [((2, blocks, 2 * n, dv), f32), ((2, blocks, 2 * n, dk), bf16)],
        flops=4 * tok * BLOCK * (dk + dv),
    )

    gates = gate_proj.reshape(8, 2, n, dv)
    bases = residual.reshape(16, n, width)
    normed, ups = [None, None], [None, None]
    for k in (1, 0):
        shape = ((4, n, width), bf16)
        keep, send = call(
            functools.partial(heads_kernel, chunk=k), sc,
            (log, *incoming, prefix, within, scaled, gates, out_weight), [shape, shape],
            scratch=[pltpu.VMEM((dk, dv), f32)], flops=tok * dv * (dk + width),
        )
        normed[k] = reduce_and_norm(sc, keep, send, bases, norm_gain, norm_bias, 0, k)
    for k in (1, 0):
        ups[k] = up_project(sc, gather_rows(normed[k]), weights, 2 * hidden)
    last = ups[1][8 * n - 16 :]
    edge = lax.ppermute(last, SP, [(i, i + 1) for i in range(15)])
    outs = []
    for k in (0, 1):
        keep, send = down_project(sc, ups[k], ups[1 - k], edge, taps, bias, weights, width, k)
        outs.append(reduce_and_norm(sc, keep, send, normed[k][None], norm_gain, norm_bias, 1, None))
    return jnp.concatenate(outs, axis=0)


def solution(mesh):
    torus = Mesh(mesh.devices.reshape(4, 4, 4, 2), SP + TP)
    return jax.shard_map(
        shards,
        mesh=torus,
        in_specs=(
            P(SP, TP),
            P(SP, TP),
            P(SP, TP),
            P(SP, TP),
            P(SP, TP),
            P(SP, None),
            P(TP, None),
            P(),
            P(),
            P(SP, TP),
            P(SP, TP),
            P(None, None, TP),
            P(None, TP),
            P(TP, SP),
        ),
        out_specs=P(SP + TP, None),
        check_vma=False,
    )
```

```python
import functools

import jax
import jax.numpy as jnp
import numpy as np
from jax import lax
from jax.experimental import pallas as pl
from jax.experimental.pallas import tpu as pltpu
from jax.sharding import Mesh
from jax.sharding import PartitionSpec as P


BLOCK = 256
SP = ("z", "y")
TP = ("x", "c")
f32 = jnp.float32
bf16 = jnp.bfloat16

ALPHA = 8.0**0.25
ROPE_BASE = 10000.0
EPS = 1e-05
EXTRA = 16
HIGHEST = lax.Precision.HIGHEST


def ring(shift, size=4):
    return [(i, (i + shift) % size) for i in range(size)]


def shift_by(x, axis, by):
    return lax.ppermute(x, axis, ring(by))


def everyone(x, axis):
    return [x] + [shift_by(x, axis, d) for d in (1, 2, 3)]


def swap_cores(x):
    return lax.ppermute(x, "c", [(0, 1), (1, 0)])


def run(kernel, sc, args, outs, scratch=(), flops=0, limit=8, far=0, far_outs=0):
    near, away = pl.BlockSpec(memory_space=pltpu.VMEM), pl.BlockSpec(memory_space=pltpu.HBM)
    split, kept = len(args) - far, len(outs) - far_outs
    args = [pltpu.with_memory_space_constraint(a, pltpu.VMEM if i < split else pltpu.HBM) for i, a in enumerate(args)]
    spaces = [pltpu.VMEM] * kept + [pltpu.HBM] * far_outs
    return pl.pallas_call(
        kernel,
        in_specs=[pl.BlockSpec(memory_space=pltpu.SMEM)] + [near] * split + [away] * far,
        out_specs=[near] * kept + [away] * far_outs,
        out_shape=[space(shape, dtype) for space, (shape, dtype) in zip(spaces, outs)],
        scratch_shapes=scratch,
        cost_estimate=pl.CostEstimate(flops=flops, transcendentals=0, bytes_accessed=0),
        compiler_params=pltpu.CompilerParams(vmem_limit_bytes=limit << 20),
    )(sc, *args)


def trig_tables(half, rows, count):
    freq = ROPE_BASE ** (-2.0 * np.arange(half, dtype=np.float64) / (2 * half))
    low = np.arange(rows, dtype=np.float64)[:, None] * freq[None, :]
    high = rows * np.arange(count, dtype=np.float64)[:, None] * freq[None, :]
    return np.stack([np.cos(low), np.sin(low), np.cos(high), np.sin(high)]).astype(np.float32)


def angles(at, tables):
    high_cos, high_sin = tables[2, pl.ds(at, 1), :], tables[3, pl.ds(at, 1), :]
    cos = high_cos * tables[0] - high_sin * tables[1]
    return cos, high_sin * tables[0] + high_cos * tables[1]


def rotated(x, cos, sin):
    half = cos.shape[1]
    front, second = x[:, :half], x[:, half:]
    return jnp.concatenate([front * cos - second * sin, front * sin + second * cos], axis=1)


def triangle(n):
    r = lax.broadcasted_iota(jnp.int32, (n, n), 0)
    c = lax.broadcasted_iota(jnp.int32, (n, n), 1)
    return r >= c


def running_logs(row, lower):
    n = lower.shape[0]
    rows = jnp.broadcast_to(row, (8, n))
    tri = lower.astype(f32)
    down = lax.dot_general(tri, rows, (((1,), (1,)), ((), ())), precision=HIGHEST, preferred_element_type=f32)
    across = lax.dot_general(rows, tri, (((1,), (1,)), ((), ())), precision=HIGHEST, preferred_element_type=f32)
    return down[:, 0:1], across[0:1, :]


def log_rows(total, width):
    a = total.astype(bf16)
    b = (total - a.astype(f32)).astype(bf16)
    c = (total - a.astype(f32) - b.astype(f32)).astype(bf16)
    at = lax.broadcasted_iota(jnp.int32, (EXTRA, width), 0)
    pick = jnp.where(at == 0, a.astype(f32), jnp.where(at == 1, b.astype(f32), c.astype(f32)))
    return jnp.where(at < 3, pick, 0.0).astype(bf16)


def log_of(rows):
    return rows[0:1, 0:1] + rows[1:2, 0:1] + rows[2:3, 0:1]


def states_kernel(sc, log, k, v, tables, kr, cosine, sine, prefix, p0, p1, p2, p3, state):
    lower = triangle(BLOCK)
    state[...] = jnp.zeros_like(state)

    def step(b, _):
        at = pl.ds(pl.multiple_of(b * BLOCK, BLOCK), BLOCK)
        cum, _ = running_logs(log[:, at], lower)
        total = cum[BLOCK - 1 : BLOCK, :]
        span = tables.shape[1]
        for i in range(BLOCK // span):
            turn = angles((4 * sc[0] + sc[1]) * (tables.shape[1] // 16) + b * (BLOCK // span) + i, tables)
            here = pl.ds(pl.multiple_of(b * BLOCK + i * span, span), span)
            cosine[here, :], sine[here, :] = turn
        key = rotated(k[at, :].astype(f32), cosine[at, :], sine[at, :]) * k.shape[1] ** (-0.5)
        key = key.astype(bf16)
        kr[at, :] = key
        faded = (key.astype(f32) * jnp.exp(total - cum)).astype(bf16)
        add = lax.dot_general(faded, v[at, :], (((0,), (0,)), ((), ())), preferred_element_type=f32)
        prefix[b] = state[...].astype(bf16)
        state[...] = jnp.exp(total) * state[...] + add
        return 0

    lax.fori_loop(0, log.shape[1] // BLOCK, step, 0)
    everything = jnp.sum(log[...], axis=1, keepdims=True)
    tail = log_rows(everything, state.shape[1])
    rows = state.shape[0] // 4
    for d, out in enumerate((p0, p1, p2, p3)):
        at = pl.multiple_of(lax.rem(sc[1] + d, 4) * rows, rows)
        out[:rows] = state[pl.ds(at, rows), :].astype(bf16)
        out[rows:] = tail


def line_kernel(sc, r0, r1, r2, r3, total, entry, logs, pieces):
    rows = entry.shape[1]
    for d, r in enumerate((r0, r1, r2, r3)):
        pieces[lax.rem(sc[1] + 4 - d, 4)] = r[...]
    run = jnp.zeros(entry.shape[1:], f32)
    passed = jnp.zeros((1, 1), f32)
    for j in range(4):
        entry[j] = run
        logs[j : j + 1, :] = jnp.broadcast_to(passed, (1, logs.shape[1]))
        here = log_of(pieces[j, rows:].astype(f32))
        run = jnp.exp(here) * run + pieces[j, :rows].astype(f32)
        passed = passed + here
    total[:rows] = run.astype(bf16)
    total[rows:] = log_rows(passed, total.shape[1])


def incoming_kernel(sc, t1, t2, t3, entry, logs, o0, o1, o2, o3):
    rows = entry.shape[1]
    run = jnp.zeros(entry.shape[1:], f32)
    for d, t in ((3, t3), (2, t2), (1, t1)):
        new = jnp.exp(log_of(t[rows:].astype(f32))) * run + t[:rows].astype(f32)
        run = jnp.where(sc[0] >= d, new, run)
    for d, out in enumerate((o0, o1, o2, o3)):
        at = lax.rem(sc[1] + d, 4)
        fade = jnp.exp(logs[pl.ds(at, 1), 0:1])
        out[...] = (fade * run + entry[at]).astype(bf16)


def within_kernel(sc, log, kr, cosine, sine, prefix, q, v, within, scaled):
    lower = triangle(BLOCK)
    n = BLOCK // 4

    def step(b, _):
        at = pl.ds(pl.multiple_of(b * BLOCK, BLOCK), BLOCK)
        cum, across = running_logs(log[:, at], lower)
        query = rotated(q[at, :].astype(f32), cosine[at, :], sine[at, :]).astype(bf16)
        score = lax.dot_general(query, kr[at, :], (((1,), (1,)), ((), ())), preferred_element_type=f32)
        weight = jnp.where(lower, jnp.exp(jnp.where(lower, cum - across, 0.0)), 0.0)
        result = jnp.dot((score * weight).astype(bf16), v[at, :], preferred_element_type=f32)
        faded = (query.astype(f32) * jnp.exp(cum)).astype(bf16)
        result = result + jnp.dot(faded, prefix[b], preferred_element_type=f32)
        for i in range(4):
            to = pl.ds(pl.multiple_of((2 * b + i // 2) * n, n), n)
            within[i % 2, to, :] = result[i * n : (i + 1) * n]
            scaled[i % 2, to, :] = faded[i * n : (i + 1) * n]
        return 0

    lax.fori_loop(0, log.shape[1] // BLOCK, step, 0)


def heads_kernel(sc, log, i0, i1, i2, i3, within, scaled, gate, weight, keep, send, start, carried, chunk):
    rows = i0.shape[0]
    for d, piece in enumerate((i0, i1, i2, i3)):
        at = pl.multiple_of(lax.rem(sc[1] + 4 - d, 4) * rows, rows)
        start[pl.ds(at, rows), :] = piece[...]
    order = lax.broadcasted_iota(jnp.int32, log.shape, 1)
    n = keep.shape[1]
    south = sc[3] == 0
    carried[...] = jnp.dot(scaled[chunk], start[...], preferred_element_type=f32)
    gated = []
    for b in range(log.shape[1] // BLOCK):
        passed = jnp.sum(jnp.where(order < b * BLOCK, log[...], 0.0), axis=1, keepdims=True)
        at = slice(2 * b * n, 2 * (b + 1) * n)
        mixed = within[chunk, at, :] + jnp.exp(passed) * carried[at, :]
        centred = mixed - jnp.mean(mixed, axis=1, keepdims=True)
        spread = jnp.mean(centred * centred, axis=1, keepdims=True)
        g = jnp.concatenate([gate[2 * b, chunk], gate[2 * b + 1, chunk]], axis=0).astype(f32)
        gated.append((g * jax.nn.sigmoid(g) * (centred * lax.rsqrt(spread + EPS))).astype(bf16))
    gated = jnp.concatenate(gated, axis=0)
    place(keep, send, sc, south, lambda cols: jnp.dot(gated, weight[:, cols], preferred_element_type=f32))


def place(keep, send, sc, south, product, tile=512):
    n = keep.shape[1]
    for j in range(keep.shape[2] // tile):
        cols = slice(j * tile, (j + 1) * tile)
        part = product(cols).astype(bf16)
        for xx in range(4):
            lo, hi = part[2 * xx * n : (2 * xx + 1) * n], part[(2 * xx + 1) * n : (2 * xx + 2) * n]
            at = lax.rem(xx + 4 - sc[2], 4)
            keep[at, :, cols] = jnp.where(south, lo, hi)
            send[at, :, cols] = jnp.where(south, hi, lo)


def scatter_kernel(sc, keep, got, s1, s2, s3):
    for d, out in ((1, s1), (2, s2), (3, s3)):
        out[...] = (keep[d].astype(f32) + got[d].astype(f32)).astype(bf16)


def norm_kernel(sc, keep, got, r1, r2, r3, base, gain, shift, *rest, row, group):
    out, rows = rest[-1], keep.shape[1]
    total = keep[0].astype(f32) + got[0].astype(f32) + r1[...].astype(f32)
    total = total + r2[...].astype(f32) + r3[...].astype(f32)
    at = 0 if group is None else 4 * sc[2] + 2 * sc[3] + group
    total = total + ALPHA * base[at].astype(f32)
    centred = total - jnp.mean(total, axis=1, keepdims=True)
    spread = jnp.mean(centred * centred, axis=1, keepdims=True)
    if len(rest) > 1:
        out[rows:] = rest[0][...]
    out[:rows] = (
        centred * lax.rsqrt(spread + EPS) * gain[row : row + 1, :] + shift[row : row + 1, :]
    ).astype(bf16)


def reduce_and_norm(sc, keep, send, base, gain, shift, row, group, *after):
    _, rows, width = keep.shape
    piece = ((rows, width), bf16)
    got = swap_cores(send)
    size = rows * width
    sums = run(scatter_kernel, sc, (keep, got), [piece] * 3, flops=size * 400)
    far = [shift_by(s, "x", d) for d, s in zip((1, 2, 3), sums)]
    return run(
        functools.partial(norm_kernel, row=row, group=group),
        sc, (keep, got, *far, base, gain, shift, *after), [((rows * (1 + len(after)), width), bf16)], flops=size * 400,
    )[0]


def gather_rows(own):
    mine = everyone(own, "x")
    return mine + [swap_cores(m) for m in mine]


def opening_kernel(sc, *refs):
    sources, gate, value, down = refs[:5], *refs[5:8]
    homes, shard = refs[8:13], refs[13]
    gate_v, value_v, down_v, both, sems, weight_sems = refs[14:]
    loads = [
        pltpu.make_async_copy(src, dst, weight_sems.at[i])
        for i, (src, dst) in enumerate(((gate, gate_v), (value, value_v), (down, down_v)))
    ]
    moves = [pltpu.make_async_copy(src, dst, sems.at[i]) for i, (src, dst) in enumerate(zip(sources, homes))]
    for copy in loads + moves:
        copy.start()
    for copy in loads:
        copy.wait()
    parts = [r[...].astype(f32).T for r in (gate_v, value_v, down_v)]
    rest = both.shape[1] - sum(p.shape[1] for p in parts)
    both[...] = jnp.concatenate(parts + [jnp.zeros((both.shape[0], rest), f32)], axis=1).astype(bf16)
    out = pltpu.make_async_copy(both, shard, weight_sems.at[3])
    out.start()
    for copy in moves:
        copy.wait()
    out.wait()


def gather_into(sc, pieces, rows):
    n = pieces[0].shape[0]
    for i, piece in enumerate(pieces):
        core = sc[3] if i < 4 else 1 - sc[3]
        at = pl.multiple_of((2 * lax.rem(sc[2] + 4 - i % 4, 4) + core) * n, n)
        rows[pl.ds(at, n), :] = piece[...]


def first_up_kernel(sc, *refs):
    pieces, weight, out, up, down, rows, total, sems = refs[:8], *refs[8:]
    steps = sems.shape[0] - 1
    deep = up.shape[0] // steps
    parts = [slice(i * deep, (i + 1) * deep) for i in range(steps)]
    loads = [
        pltpu.make_async_copy(weight.at[p, pl.ds(0, up.shape[1])], up.at[p], sems.at[i]) for i, p in enumerate(parts)
    ]
    loads.append(pltpu.make_async_copy(weight.at[:, pl.ds(up.shape[1], down.shape[1])], down, sems.at[steps]))
    for load in loads:
        load.start()
    gather_into(sc, pieces, rows)
    for i, p in enumerate(parts):
        loads[i].wait()
        part = jnp.dot(rows[:, p], up[p, :], preferred_element_type=f32)
        if i == 0:
            total[...] = part
        elif i < steps - 1:
            total[...] += part
        else:
            out[...] = (total[...] + part).astype(bf16)
    loads[steps].wait()


def second_up_kernel(sc, *refs):
    pieces, weight, out, rows = refs[:8], *refs[8:]
    gather_into(sc, pieces, rows)
    out[...] = jnp.dot(rows[...], weight[...], preferred_element_type=f32).astype(bf16)


def first_up(sc, pieces, weights, hidden):
    n, width = pieces[0].shape
    return run(
        first_up_kernel, sc, (*pieces, weights),
        [((8 * n, hidden), bf16), ((width, hidden), bf16), ((width, weights.shape[1] - hidden), bf16)],
        scratch=[
            pltpu.VMEM((8 * n, width), bf16), pltpu.VMEM((8 * n, hidden), f32), pltpu.SemaphoreType.DMA((5,))
        ],
        flops=16 * n * width * hidden, limit=16, far=1,
    )


def second_up(sc, pieces, weights, hidden):
    n, width = pieces[0].shape
    return run(
        second_up_kernel, sc, (*pieces, weights), [((8 * n, hidden), bf16)],
        scratch=[pltpu.VMEM((8 * n, width), bf16)], flops=16 * n * width * hidden, limit=16,
    )[0]


def down_kernel(sc, mine, other, edge, taps, bias, weight, keep, send, active, padded, chunk):
    n = keep.shape[1]
    hidden = active.shape[1]

    def conv_group(t, _):
        at = pl.multiple_of(t * n, n)
        if chunk == 1:
            halo = other[pl.ds(pl.multiple_of(at + n - 16, 16), 16), :][8:]
        else:
            before = pl.multiple_of(jnp.maximum(at - 16, 0), 16)
            halo = jnp.where(t == 0, edge[8:].astype(f32), other[pl.ds(before, 16), :][8:].astype(f32))
        padded[0:8] = halo.astype(f32)
        padded[8:] = mine[pl.ds(at, n), :].astype(f32)
        conv = bias[0:1, :] + padded[6 : 6 + n] * taps[0:1, :]
        conv = conv + padded[7 : 7 + n] * taps[1:2, :]
        conv = conv + padded[8 : 8 + n] * taps[2:3, :]
        active[pl.ds(at, n), :] = (jax.nn.gelu(conv[:, :hidden]) * conv[:, hidden:]).astype(bf16)
        return 0

    lax.fori_loop(0, 8, conv_group, 0)
    place(keep, send, sc, sc[3] == 0, lambda cols: lax.dot_general(
        active[...], weight[cols, :hidden], (((1,), (1,)), ((), ())), preferred_element_type=f32
    ))


def down_project(sc, mine, other, edge, taps, bias, weights, width, chunk):
    rows, double = mine.shape
    n = rows // 8
    shape = ((4, n, width), bf16)
    return run(
        functools.partial(down_kernel, chunk=chunk), sc,
        (mine, other, edge, taps, bias, weights), [shape, shape],
        scratch=[pltpu.VMEM((rows, double // 2), bf16), pltpu.VMEM((n + 8, double), f32)],
        flops=rows * width * double * 2, limit=16,
    )


def shards(
    query_proj, key_proj, value_proj, gate_proj, log_decay, residual, out_weight, norm_gain,
    norm_bias, up_gate, up_value, conv_weight, conv_bias, down_weight,
):
    tok, dk = query_proj.shape
    dv = value_proj.shape[1]
    width = residual.shape[1]
    hidden = up_gate.shape[1]
    blocks = tok // BLOCK
    n = tok // 16
    taps = jnp.concatenate([conv_weight[0], conv_weight[1]], axis=1)
    bias = jnp.concatenate([conv_bias[0:1], conv_bias[1:2]], axis=1)
    sc = jnp.stack([lax.axis_index(a) for a in ("z", "y", "x", "c")]).astype(jnp.int32)

    tables = jnp.asarray(trig_tables(dk // 2, 128, 128))
    padded = -(-3 * hidden // 128) * 128
    near = (log_decay.T, query_proj, key_proj, value_proj, tables)
    column = ((hidden, up_gate.shape[0]), bf16)
    log, query, key, value, tables, shard = run(
        opening_kernel, sc, (*near, up_gate.T, up_value.T, down_weight),
        [(a.shape, a.dtype) for a in near] + [((up_gate.shape[0], padded), bf16)],
        scratch=[pltpu.VMEM(*column)] * 3
        + [pltpu.VMEM((up_gate.shape[0], padded), bf16), pltpu.SemaphoreType.DMA((5,)), pltpu.SemaphoreType.DMA((4,))],
        flops=1 << 26, far=8, far_outs=1,
    )
    weights = lax.all_gather(shard, SP, axis=0, tiled=True)
    piece = ((dk // 4 + EXTRA, dv), bf16)
    turn = ((tok, dk // 2), f32)
    key_rot, cosine, sine, prefix, *pieces = run(
        states_kernel, sc, (log, key, value, tables),
        [((tok, dk), bf16), turn, turn, ((blocks, dk, dv), bf16)] + [piece] * 4,
        scratch=[pltpu.VMEM((dk, dv), f32)], flops=4 * tok * dk * dv,
    )
    got = [pieces[0]] + [shift_by(pieces[d], "y", d) for d in (1, 2, 3)]
    within, scaled = run(
        within_kernel, sc, (log, key_rot, cosine, sine, prefix, query, value),
        [((2, tok // 2, dv), f32), ((2, tok // 2, dk), bf16)],
        flops=4 * tok * BLOCK * (dk + dv),
    )
    total, entry, logs = run(
        line_kernel, sc, got, [piece, ((4, dk // 4, dv), f32), ((8, 128), f32)],
        scratch=[pltpu.VMEM((4,) + piece[0], bf16)], flops=100 * dk * dv,
    )
    lines = everyone(total, "z")[1:]
    quarter = ((dk // 4, dv), bf16)
    outgoing = run(incoming_kernel, sc, (*lines, entry, logs), [quarter] * 4, flops=100 * dk * dv)
    incoming = [outgoing[0]] + [shift_by(outgoing[d], "y", d) for d in (1, 2, 3)]
    gates = gate_proj.reshape(8, 2, n, dv)
    bases = residual.reshape(16, n, width)
    normed, ups, rows = [None, None], [None, None], [None, None]
    for k in (1, 0):
        shape = ((4, n, width), bf16)
        keep, send = run(
            functools.partial(heads_kernel, chunk=k), sc,
            (log, *incoming, within, scaled, gates, out_weight), [shape, shape],
            scratch=[pltpu.VMEM((dk, dv), bf16), pltpu.VMEM((tok // 2, dv), f32)], flops=tok * dv * (dk + width),
        )
        normed[k] = reduce_and_norm(sc, keep, send, bases, norm_gain, norm_bias, 0, k)
        rows[k] = gather_rows(normed[k])
    ups[1], weights, down_weights = first_up(sc, rows[1], weights, 2 * hidden)
    ups[0] = second_up(sc, rows[0], weights, 2 * hidden)
    edge = lax.ppermute(ups[1][8 * n - 16 :], SP, [(i, i + 1) for i in range(15)])
    outs = [None, None]
    for k in (1, 0):
        keep, send = down_project(sc, ups[k], ups[1 - k], edge, taps, bias, down_weights, width, k)
        outs[k] = reduce_and_norm(sc, keep, send, normed[k][None], norm_gain, norm_bias, 1, None, *outs[k + 1 :])
    return outs[0]


def solution(mesh):
    torus = Mesh(mesh.devices.reshape(4, 4, 4, 2), SP + TP)
    return jax.shard_map(
        shards,
        mesh=torus,
        in_specs=(
            P(SP, TP),
            P(SP, TP),
            P(SP, TP),
            P(SP, TP),
            P(SP, TP),
            P(SP, None),
            P(TP, None),
            P(),
            P(),
            P(SP, TP),
            P(SP, TP),
            P(None, None, TP),
            P(None, TP),
            P(TP, SP),
        ),
        out_specs=P(SP + TP, None),
        check_vma=False,
    )
```

```python
import functools

import jax
import jax.numpy as jnp
import numpy as np
from jax import lax
from jax.experimental import pallas as pl
from jax.experimental.pallas import tpu as pltpu
from jax.sharding import Mesh
from jax.sharding import PartitionSpec as P


BLOCK = 256
SP = ("z", "y")
TP = ("x", "c")
f32 = jnp.float32
bf16 = jnp.bfloat16

ALPHA = 8.0**0.25
ROPE_BASE = 10000.0
EPS = 1e-05
EXTRA = 16


def ring(shift, size=4):
    return [(i, (i + shift) % size) for i in range(size)]


def shift_by(x, axis, by):
    return lax.ppermute(x, axis, ring(by))


def everyone(x, axis):
    return [x] + [shift_by(x, axis, d) for d in (1, 2, 3)]


def swap_cores(x):
    return lax.ppermute(x, "c", [(0, 1), (1, 0)])


def run(kernel, sc, args, outs, scratch=(), flops=0, limit=8, far=0, far_outs=0):
    near, away = pl.BlockSpec(memory_space=pltpu.VMEM), pl.BlockSpec(memory_space=pltpu.HBM)
    split, kept = len(args) - far, len(outs) - far_outs
    args = [pltpu.with_memory_space_constraint(a, pltpu.VMEM if i < split else pltpu.HBM) for i, a in enumerate(args)]
    spaces = [pltpu.VMEM] * kept + [pltpu.HBM] * far_outs
    return pl.pallas_call(
        kernel,
        in_specs=[pl.BlockSpec(memory_space=pltpu.SMEM)] + [near] * split + [away] * far,
        out_specs=[near] * kept + [away] * far_outs,
        out_shape=[space(shape, dtype) for space, (shape, dtype) in zip(spaces, outs)],
        scratch_shapes=scratch,
        cost_estimate=pl.CostEstimate(flops=flops, transcendentals=0, bytes_accessed=0),
        compiler_params=pltpu.CompilerParams(vmem_limit_bytes=limit << 20),
    )(sc, *args)


def trig_tables(half, rows, count):
    freq = ROPE_BASE ** (-2.0 * np.arange(half, dtype=np.float64) / (2 * half))
    low = np.arange(rows, dtype=np.float64)[:, None] * freq[None, :]
    high = rows * np.arange(count, dtype=np.float64)[:, None] * freq[None, :]
    return np.stack([np.cos(low), np.sin(low), np.cos(high), np.sin(high)]).astype(np.float32)


def angles(at, tables):
    high_cos, high_sin = tables[2, pl.ds(at, 1), :], tables[3, pl.ds(at, 1), :]
    cos = high_cos * tables[0] - high_sin * tables[1]
    return cos, high_sin * tables[0] + high_cos * tables[1]


def rotated(x, cos, sin):
    half = cos.shape[1]
    front, second = x[:, :half], x[:, half:]
    return jnp.concatenate([front * cos - second * sin, front * sin + second * cos], axis=1)


def triangle(n):
    r = lax.broadcasted_iota(jnp.int32, (n, n), 0)
    c = lax.broadcasted_iota(jnp.int32, (n, n), 1)
    return r >= c


def split_logs(log):
    blocks = log.shape[1] // BLOCK
    whole = jnp.concatenate([log[:, b * BLOCK : (b + 1) * BLOCK] for b in range(blocks)], axis=0)
    first = whole.astype(bf16).astype(f32)
    second = (whole - first).astype(bf16).astype(f32)
    third = whole - first - second
    return jnp.concatenate([first, second, third, jnp.zeros_like(whole)], axis=0).astype(bf16)


def running_logs(log, down, across):
    terms = split_logs(log[...])
    lower = triangle(BLOCK).astype(f32).astype(bf16)
    last = (((1,), (1,)), ((), ()))
    down[...] = lax.dot_general(lower, terms, last, preferred_element_type=f32)
    across[...] = lax.dot_general(terms, lower, last, preferred_element_type=f32)


def log_column(down, b):
    lane = lax.broadcasted_iota(jnp.int32, down.shape, 1)
    blocks = down.shape[1] // 4
    mine = (lane == b) | (lane == b + blocks) | (lane == b + 2 * blocks)
    return jnp.sum(jnp.where(mine, down[...], 0.0), axis=1, keepdims=True)


def log_row(across, b):
    blocks = across.shape[0] // 4
    return across[pl.ds(b, 1), :] + across[pl.ds(b + blocks, 1), :] + across[pl.ds(b + 2 * blocks, 1), :]


def log_rows(total, width):
    a = total.astype(bf16)
    b = (total - a.astype(f32)).astype(bf16)
    c = (total - a.astype(f32) - b.astype(f32)).astype(bf16)
    at = lax.broadcasted_iota(jnp.int32, (EXTRA, width), 0)
    pick = jnp.where(at == 0, a.astype(f32), jnp.where(at == 1, b.astype(f32), c.astype(f32)))
    return jnp.where(at < 3, pick, 0.0).astype(bf16)


def log_of(rows):
    return rows[0:1, 0:1] + rows[1:2, 0:1] + rows[2:3, 0:1]


def states_kernel(sc, log, k, v, tables, kr, cosine, sine, prefix, down, across, p0, p1, p2, p3, state):
    running_logs(log, down, across)
    state[...] = jnp.zeros_like(state)

    def step(b, _):
        at = pl.ds(pl.multiple_of(b * BLOCK, BLOCK), BLOCK)
        cum = log_column(down, b)
        total = cum[BLOCK - 1 : BLOCK, :]
        span = tables.shape[1]
        for i in range(BLOCK // span):
            turn = angles((4 * sc[0] + sc[1]) * (tables.shape[1] // 16) + b * (BLOCK // span) + i, tables)
            here = pl.ds(pl.multiple_of(b * BLOCK + i * span, span), span)
            cosine[here, :], sine[here, :] = turn
        key = rotated(k[at, :].astype(f32), cosine[at, :], sine[at, :]) * k.shape[1] ** (-0.5)
        key = key.astype(bf16)
        kr[at, :] = key
        faded = (key.astype(f32) * jnp.exp(total - cum)).astype(bf16)
        add = lax.dot_general(faded, v[at, :], (((0,), (0,)), ((), ())), preferred_element_type=f32)
        prefix[b] = state[...].astype(bf16)
        state[...] = jnp.exp(total) * state[...] + add
        return 0

    lax.fori_loop(0, log.shape[1] // BLOCK, step, 0)
    everything = jnp.sum(log[...], axis=1, keepdims=True)
    tail = log_rows(everything, state.shape[1])
    rows = state.shape[0] // 4
    for d, out in enumerate((p0, p1, p2, p3)):
        at = pl.multiple_of(lax.rem(sc[1] + d, 4) * rows, rows)
        out[:rows] = state[pl.ds(at, rows), :].astype(bf16)
        out[rows:] = tail


def line_kernel(sc, r0, r1, r2, r3, total, entry, logs, pieces):
    rows = entry.shape[1]
    for d, r in enumerate((r0, r1, r2, r3)):
        pieces[lax.rem(sc[1] + 4 - d, 4)] = r[...]
    run = jnp.zeros(entry.shape[1:], f32)
    passed = jnp.zeros((1, 1), f32)
    for j in range(4):
        entry[j] = run
        logs[j : j + 1, :] = jnp.broadcast_to(passed, (1, logs.shape[1]))
        here = log_of(pieces[j, rows:].astype(f32))
        run = jnp.exp(here) * run + pieces[j, :rows].astype(f32)
        passed = passed + here
    total[:rows] = run.astype(bf16)
    total[rows:] = log_rows(passed, total.shape[1])


def incoming_kernel(sc, t1, t2, t3, entry, logs, o0, o1, o2, o3):
    rows = entry.shape[1]
    run = jnp.zeros(entry.shape[1:], f32)
    for d, t in ((3, t3), (2, t2), (1, t1)):
        new = jnp.exp(log_of(t[rows:].astype(f32))) * run + t[:rows].astype(f32)
        run = jnp.where(sc[0] >= d, new, run)
    for d, out in enumerate((o0, o1, o2, o3)):
        at = lax.rem(sc[1] + d, 4)
        fade = jnp.exp(logs[pl.ds(at, 1), 0:1])
        out[...] = (fade * run + entry[at]).astype(bf16)


def within_kernel(sc, down, across, kr, cosine, sine, prefix, q, v, within, scaled):
    lower = triangle(BLOCK)
    n = BLOCK // 4

    def step(b, _):
        at = pl.ds(pl.multiple_of(b * BLOCK, BLOCK), BLOCK)
        cum, row = log_column(down, b), log_row(across, b)
        query = rotated(q[at, :].astype(f32), cosine[at, :], sine[at, :]).astype(bf16)
        score = lax.dot_general(query, kr[at, :], (((1,), (1,)), ((), ())), preferred_element_type=f32)
        weight = jnp.where(lower, jnp.exp(jnp.where(lower, cum - row, 0.0)), 0.0)
        result = jnp.dot((score * weight).astype(bf16), v[at, :], preferred_element_type=f32)
        faded = (query.astype(f32) * jnp.exp(cum)).astype(bf16)
        result = result + jnp.dot(faded, prefix[b], preferred_element_type=f32)
        for i in range(4):
            to = pl.ds(pl.multiple_of((2 * b + i // 2) * n, n), n)
            within[i % 2, to, :] = result[i * n : (i + 1) * n]
            scaled[i % 2, to, :] = faded[i * n : (i + 1) * n]
        return 0

    lax.fori_loop(0, kr.shape[0] // BLOCK, step, 0)


def heads_kernel(sc, log, i0, i1, i2, i3, within, scaled, gate, weight, keep, send, start, carried, chunk):
    rows = i0.shape[0]
    for d, piece in enumerate((i0, i1, i2, i3)):
        at = pl.multiple_of(lax.rem(sc[1] + 4 - d, 4) * rows, rows)
        start[pl.ds(at, rows), :] = piece[...]
    order = lax.broadcasted_iota(jnp.int32, log.shape, 1)
    n = keep.shape[1]
    south = sc[3] == 0
    carried[...] = jnp.dot(scaled[chunk], start[...], preferred_element_type=f32)
    gated = []
    for b in range(log.shape[1] // BLOCK):
        passed = jnp.sum(jnp.where(order < b * BLOCK, log[...], 0.0), axis=1, keepdims=True)
        at = slice(2 * b * n, 2 * (b + 1) * n)
        mixed = within[chunk, at, :] + jnp.exp(passed) * carried[at, :]
        centred = mixed - jnp.mean(mixed, axis=1, keepdims=True)
        spread = jnp.mean(centred * centred, axis=1, keepdims=True)
        g = jnp.concatenate([gate[2 * b, chunk], gate[2 * b + 1, chunk]], axis=0).astype(f32)
        gated.append((g * jax.nn.sigmoid(g) * (centred * lax.rsqrt(spread + EPS))).astype(bf16))
    gated = jnp.concatenate(gated, axis=0)
    place(keep, send, sc, south, lambda cols: jnp.dot(gated, weight[:, cols], preferred_element_type=f32))


def place(keep, send, sc, south, product, tile=512):
    n = keep.shape[1]
    for j in range(keep.shape[2] // tile):
        cols = slice(j * tile, (j + 1) * tile)
        part = product(cols).astype(bf16)
        for xx in range(4):
            lo, hi = part[2 * xx * n : (2 * xx + 1) * n], part[(2 * xx + 1) * n : (2 * xx + 2) * n]
            at = lax.rem(xx + 4 - sc[2], 4)
            keep[at, :, cols] = jnp.where(south, lo, hi)
            send[at, :, cols] = jnp.where(south, hi, lo)


def scatter_kernel(sc, keep, got, s1, s2, s3):
    for d, out in ((1, s1), (2, s2), (3, s3)):
        out[...] = (keep[d].astype(f32) + got[d].astype(f32)).astype(bf16)


def norm_kernel(sc, keep, got, r1, r2, r3, base, gain, shift, *rest, row, group):
    out, rows = rest[0], keep.shape[1]
    total = keep[0].astype(f32) + got[0].astype(f32) + r1[...].astype(f32)
    total = total + r2[...].astype(f32) + r3[...].astype(f32)
    at = 0 if group is None else 4 * sc[2] + 2 * sc[3] + group
    total = total + ALPHA * base[at].astype(f32)
    centred = total - jnp.mean(total, axis=1, keepdims=True)
    spread = jnp.mean(centred * centred, axis=1, keepdims=True)
    if len(rest) > 1:
        after, target, own, sems = rest
        later = pltpu.make_async_copy(after, target.at[pl.ds(rows, after.shape[0])], sems.at[1])
        later.start()
    result = (
        centred * lax.rsqrt(spread + EPS) * gain[row : row + 1, :] + shift[row : row + 1, :]
    ).astype(bf16)
    if len(rest) == 1:
        out[...] = result
        return
    own[...] = result
    mine = pltpu.make_async_copy(own, target.at[pl.ds(0, rows)], sems.at[0])
    mine.start()
    mine.wait()
    later.wait()


def reduce_and_norm(sc, keep, send, base, gain, shift, row, group, *after):
    _, rows, width = keep.shape
    piece = ((rows, width), bf16)
    got = swap_cores(send)
    size = rows * width
    sums = run(scatter_kernel, sc, (keep, got), [piece] * 3, flops=size * 400)
    far = [shift_by(s, "x", d) for d, s in zip((1, 2, 3), sums)]
    return run(
        functools.partial(norm_kernel, row=row, group=group),
        sc, (keep, got, *far, base, gain, shift, *after), [((rows * (1 + len(after)), width), bf16)], flops=size * 400,
        far_outs=len(after), scratch=[pltpu.VMEM(*piece), pltpu.SemaphoreType.DMA((2,))] if after else [],
    )[0]


def gather_rows(own):
    mine = everyone(own, "x")
    return mine + [swap_cores(m) for m in mine]


def opening_kernel(sc, *refs):
    sources, gate, value, down = refs[:5], *refs[5:8]
    homes, shard = refs[8:13], refs[13]
    gate_v, value_v, down_v, both, sems, weight_sems = refs[14:]
    loads = [
        pltpu.make_async_copy(src, dst, weight_sems.at[i])
        for i, (src, dst) in enumerate(((gate, gate_v), (value, value_v), (down, down_v)))
    ]
    moves = [pltpu.make_async_copy(src, dst, sems.at[i]) for i, (src, dst) in enumerate(zip(sources, homes))]
    for copy in loads + moves:
        copy.start()
    for copy in loads:
        copy.wait()
    parts = [r[...] for r in (gate_v, value_v, down_v)]
    rest = both.shape[1] - sum(p.shape[0] for p in parts)
    both[...] = jnp.concatenate(parts + [jnp.zeros((rest, both.shape[0]), bf16)], axis=0).T
    out = pltpu.make_async_copy(both, shard, weight_sems.at[3])
    out.start()
    for copy in moves:
        copy.wait()
    out.wait()


def gather_into(sc, pieces, rows):
    n = pieces[0].shape[0]
    for i, piece in enumerate(pieces):
        core = sc[3] if i < 4 else 1 - sc[3]
        at = pl.multiple_of((2 * lax.rem(sc[2] + 4 - i % 4, 4) + core) * n, n)
        rows[pl.ds(at, n), :] = piece[...]


def first_up_kernel(sc, *refs):
    pieces, weight, out, up, down, rows, total, sems = refs[:8], *refs[8:]
    steps = sems.shape[0] - 1
    deep = up.shape[0] // steps
    parts = [slice(i * deep, (i + 1) * deep) for i in range(steps)]
    loads = [
        pltpu.make_async_copy(weight.at[p, pl.ds(0, up.shape[1])], up.at[p], sems.at[i]) for i, p in enumerate(parts)
    ]
    loads.append(pltpu.make_async_copy(weight.at[:, pl.ds(up.shape[1], down.shape[1])], down, sems.at[steps]))
    for load in loads:
        load.start()
    gather_into(sc, pieces, rows)
    for i, p in enumerate(parts):
        loads[i].wait()
        part = jnp.dot(rows[:, p], up[p, :], preferred_element_type=f32)
        if i == 0:
            total[...] = part
        elif i < steps - 1:
            total[...] += part
        else:
            out[...] = (total[...] + part).astype(bf16)
    loads[steps].wait()


def second_up_kernel(sc, *refs):
    pieces, weight, out, rows = refs[:8], *refs[8:]
    gather_into(sc, pieces, rows)
    out[...] = jnp.dot(rows[...], weight[...], preferred_element_type=f32).astype(bf16)


def first_up(sc, pieces, weights, hidden):
    n, width = pieces[0].shape
    return run(
        first_up_kernel, sc, (*pieces, weights),
        [((8 * n, hidden), bf16), ((width, hidden), bf16), ((width, weights.shape[1] - hidden), bf16)],
        scratch=[
            pltpu.VMEM((8 * n, width), bf16), pltpu.VMEM((8 * n, hidden), f32), pltpu.SemaphoreType.DMA((5,))
        ],
        flops=16 * n * width * hidden, limit=16, far=1,
    )


def second_up(sc, pieces, weights, hidden):
    n, width = pieces[0].shape
    return run(
        second_up_kernel, sc, (*pieces, weights), [((8 * n, hidden), bf16)],
        scratch=[pltpu.VMEM((8 * n, width), bf16)], flops=16 * n * width * hidden, limit=16,
    )[0]


def down_kernel(sc, mine, other, edge, taps, bias, weight, keep, send, active, chunk):
    n = keep.shape[1]
    hidden = active.shape[1]

    def conv_group(t, _):
        at = pl.multiple_of(t * n, n)
        if chunk == 1:
            halo = other[pl.ds(pl.multiple_of(at + n - 16, 16), 16), :][8:]
        else:
            before = pl.multiple_of(jnp.maximum(at - 16, 0), 16)
            halo = jnp.where(t == 0, edge[8:].astype(f32), other[pl.ds(before, 16), :][8:].astype(f32))
        rows = jnp.concatenate([halo.astype(f32), mine[pl.ds(at, n), :].astype(f32)], axis=0)
        conv = bias[0:1, :] + pltpu.roll(rows, 2, 0)[8:] * taps[0:1, :]
        conv = conv + pltpu.roll(rows, 1, 0)[8:] * taps[1:2, :]
        conv = conv + rows[8:] * taps[2:3, :]
        active[pl.ds(at, n), :] = (jax.nn.gelu(conv[:, :hidden]) * conv[:, hidden:]).astype(bf16)
        return 0

    lax.fori_loop(0, 8, conv_group, 0)
    place(keep, send, sc, sc[3] == 0, lambda cols: lax.dot_general(
        active[...], weight[cols, :hidden], (((1,), (1,)), ((), ())), preferred_element_type=f32
    ))


def down_project(sc, mine, other, edge, taps, bias, weights, width, chunk):
    rows, double = mine.shape
    n = rows // 8
    shape = ((4, n, width), bf16)
    return run(
        functools.partial(down_kernel, chunk=chunk), sc,
        (mine, other, edge, taps, bias, weights), [shape, shape],
        scratch=[pltpu.VMEM((rows, double // 2), bf16)],
        flops=rows * width * double * 2, limit=16,
    )


def shards(
    query_proj, key_proj, value_proj, gate_proj, log_decay, residual, out_weight, norm_gain,
    norm_bias, up_gate, up_value, conv_weight, conv_bias, down_weight,
):
    tok, dk = query_proj.shape
    dv = value_proj.shape[1]
    width = residual.shape[1]
    hidden = up_gate.shape[1]
    blocks = tok // BLOCK
    n = tok // 16
    taps = jnp.concatenate([conv_weight[0], conv_weight[1]], axis=1)
    bias = jnp.concatenate([conv_bias[0:1], conv_bias[1:2]], axis=1)
    sc = jnp.stack([lax.axis_index(a) for a in ("z", "y", "x", "c")]).astype(jnp.int32)

    tables = jnp.asarray(trig_tables(dk // 2, 128, 128))
    padded = -(-3 * hidden // 128) * 128
    near = (log_decay.T, query_proj, key_proj, value_proj, tables)
    column = ((hidden, up_gate.shape[0]), bf16)
    log, query, key, value, tables, shard = run(
        opening_kernel, sc, (*near, up_gate.T, up_value.T, down_weight),
        [(a.shape, a.dtype) for a in near] + [((up_gate.shape[0], padded), bf16)],
        scratch=[pltpu.VMEM(*column)] * 3
        + [pltpu.VMEM((up_gate.shape[0], padded), bf16), pltpu.SemaphoreType.DMA((5,)), pltpu.SemaphoreType.DMA((4,))],
        flops=1 << 26, far=8, far_outs=1,
    )
    weights = lax.all_gather(shard, SP, axis=0, tiled=True)
    piece = ((dk // 4 + EXTRA, dv), bf16)
    turn = ((tok, dk // 2), f32)
    key_rot, cosine, sine, prefix, down_logs, across_logs, *pieces = run(
        states_kernel, sc, (log, key, value, tables),
        [((tok, dk), bf16), turn, turn, ((blocks, dk, dv), bf16), ((BLOCK, 4 * blocks), f32), ((4 * blocks, BLOCK), f32)]
        + [piece] * 4,
        scratch=[pltpu.VMEM((dk, dv), f32)], flops=4 * tok * dk * dv,
    )
    got = [pieces[0]] + [shift_by(pieces[d], "y", d) for d in (1, 2, 3)]
    within, scaled = run(
        within_kernel, sc, (down_logs, across_logs, key_rot, cosine, sine, prefix, query, value),
        [((2, tok // 2, dv), f32), ((2, tok // 2, dk), bf16)],
        flops=4 * tok * BLOCK * (dk + dv),
    )
    total, entry, logs = run(
        line_kernel, sc, got, [piece, ((4, dk // 4, dv), f32), ((8, 128), f32)],
        scratch=[pltpu.VMEM((4,) + piece[0], bf16)], flops=100 * dk * dv,
    )
    lines = everyone(total, "z")[1:]
    quarter = ((dk // 4, dv), bf16)
    outgoing = run(incoming_kernel, sc, (*lines, entry, logs), [quarter] * 4, flops=100 * dk * dv)
    incoming = [outgoing[0]] + [shift_by(outgoing[d], "y", d) for d in (1, 2, 3)]
    gates = gate_proj.reshape(8, 2, n, dv)
    bases = residual.reshape(16, n, width)
    normed, ups, rows = [None, None], [None, None], [None, None]
    for k in (1, 0):
        shape = ((4, n, width), bf16)
        keep, send = run(
            functools.partial(heads_kernel, chunk=k), sc,
            (log, *incoming, within, scaled, gates, out_weight), [shape, shape],
            scratch=[pltpu.VMEM((dk, dv), bf16), pltpu.VMEM((tok // 2, dv), f32)], flops=tok * dv * (dk + width),
        )
        normed[k] = reduce_and_norm(sc, keep, send, bases, norm_gain, norm_bias, 0, k)
        rows[k] = gather_rows(normed[k])
    ups[1], weights, down_weights = first_up(sc, rows[1], weights, 2 * hidden)
    ups[0] = second_up(sc, rows[0], weights, 2 * hidden)
    edge = lax.ppermute(ups[1][8 * n - 16 :], SP, [(i, i + 1) for i in range(15)])
    outs = [None, None]
    for k in (1, 0):
        keep, send = down_project(sc, ups[k], ups[1 - k], edge, taps, bias, down_weights, width, k)
        outs[k] = reduce_and_norm(sc, keep, send, normed[k][None], norm_gain, norm_bias, 1, None, *outs[k + 1 :])
    return outs[0]


def solution(mesh):
    torus = Mesh(mesh.devices.reshape(4, 4, 4, 2), SP + TP)
    return jax.shard_map(
        shards,
        mesh=torus,
        in_specs=(
            P(SP, TP),
            P(SP, TP),
            P(SP, TP),
            P(SP, TP),
            P(SP, TP),
            P(SP, None),
            P(TP, None),
            P(),
            P(),
            P(SP, TP),
            P(SP, TP),
            P(None, None, TP),
            P(None, TP),
            P(TP, SP),
        ),
        out_specs=P(SP + TP, None),
        check_vma=False,
    )
```

```python
import functools

import jax
import jax.numpy as jnp
import numpy as np
from jax import lax
from jax.experimental import pallas as pl
from jax.experimental.pallas import tpu as pltpu
from jax.sharding import Mesh
from jax.sharding import PartitionSpec as P


BLOCK = 256
SP = ("z", "y")
TP = ("x", "c")
f32 = jnp.float32
bf16 = jnp.bfloat16

ALPHA = 8.0**0.25
ROPE_BASE = 10000.0
EPS = 1e-05
EXTRA = 16


def ring(shift, size=4):
    return [(i, (i + shift) % size) for i in range(size)]


def shift_by(x, axis, by):
    return lax.ppermute(x, axis, ring(by))


def everyone(x, axis):
    return [x] + [shift_by(x, axis, d) for d in (1, 2, 3)]


def swap_cores(x):
    return lax.ppermute(x, "c", [(0, 1), (1, 0)])


def run(kernel, sc, args, outs, scratch=(), flops=0, limit=8, far=0, far_outs=0):
    near, away = pl.BlockSpec(memory_space=pltpu.VMEM), pl.BlockSpec(memory_space=pltpu.HBM)
    split, kept = len(args) - far, len(outs) - far_outs
    args = [pltpu.with_memory_space_constraint(a, pltpu.VMEM if i < split else pltpu.HBM) for i, a in enumerate(args)]
    spaces = [pltpu.VMEM] * kept + [pltpu.HBM] * far_outs
    return pl.pallas_call(
        kernel,
        in_specs=[pl.BlockSpec(memory_space=pltpu.SMEM)] + [near] * split + [away] * far,
        out_specs=[near] * kept + [away] * far_outs,
        out_shape=[space(shape, dtype) for space, (shape, dtype) in zip(spaces, outs)],
        scratch_shapes=scratch,
        cost_estimate=pl.CostEstimate(flops=flops, transcendentals=0, bytes_accessed=0),
        compiler_params=pltpu.CompilerParams(vmem_limit_bytes=limit << 20),
    )(sc, *args)


def trig_tables(half, rows, count):
    freq = ROPE_BASE ** (-2.0 * np.arange(half, dtype=np.float64) / (2 * half))
    low = np.arange(rows, dtype=np.float64)[:, None] * freq[None, :]
    high = rows * np.arange(count, dtype=np.float64)[:, None] * freq[None, :]
    return np.stack([np.cos(low), np.sin(low), np.cos(high), np.sin(high)]).astype(np.float32)


def angles(at, tables):
    high_cos, high_sin = tables[2, pl.ds(at, 1), :], tables[3, pl.ds(at, 1), :]
    cos = high_cos * tables[0] - high_sin * tables[1]
    return cos, high_sin * tables[0] + high_cos * tables[1]


def rotated(x, cos, sin):
    half = cos.shape[1]
    front, second = x[:, :half], x[:, half:]
    return jnp.concatenate([front * cos - second * sin, front * sin + second * cos], axis=1)


def triangle(n):
    r = lax.broadcasted_iota(jnp.int32, (n, n), 0)
    c = lax.broadcasted_iota(jnp.int32, (n, n), 1)
    return r >= c


def split_logs(log):
    blocks = log.shape[1] // BLOCK
    whole = jnp.concatenate([log[:, b * BLOCK : (b + 1) * BLOCK] for b in range(blocks)], axis=0)
    first = whole.astype(bf16).astype(f32)
    second = (whole - first).astype(bf16).astype(f32)
    third = whole - first - second
    return jnp.concatenate([first, second, third, jnp.zeros_like(whole)], axis=0).astype(bf16)


def running_logs(log, down, across):
    terms = split_logs(log[...])
    lower = triangle(BLOCK).astype(f32).astype(bf16)
    last = (((1,), (1,)), ((), ()))
    down[...] = lax.dot_general(lower, terms, last, preferred_element_type=f32)
    across[...] = lax.dot_general(terms, lower, last, preferred_element_type=f32)


def log_column(down, b):
    lane = lax.broadcasted_iota(jnp.int32, down.shape, 1)
    blocks = down.shape[1] // 4
    mine = (lane == b) | (lane == b + blocks) | (lane == b + 2 * blocks)
    return jnp.sum(jnp.where(mine, down[...], 0.0), axis=1, keepdims=True)


def log_row(across, b):
    blocks = across.shape[0] // 4
    return across[pl.ds(b, 1), :] + across[pl.ds(b + blocks, 1), :] + across[pl.ds(b + 2 * blocks, 1), :]


def log_rows(total, width):
    a = total.astype(bf16)
    b = (total - a.astype(f32)).astype(bf16)
    c = (total - a.astype(f32) - b.astype(f32)).astype(bf16)
    at = lax.broadcasted_iota(jnp.int32, (EXTRA, width), 0)
    pick = jnp.where(at == 0, a.astype(f32), jnp.where(at == 1, b.astype(f32), c.astype(f32)))
    return jnp.where(at < 3, pick, 0.0).astype(bf16)


def log_of(rows):
    return rows[0:1, 0:1] + rows[1:2, 0:1] + rows[2:3, 0:1]


def states_kernel(sc, log, k, v, tables, kr, cosine, sine, prefix, down, across, p0, p1, p2, p3, state):
    running_logs(log, down, across)
    state[...] = jnp.zeros_like(state)

    def step(b, _):
        at = pl.ds(pl.multiple_of(b * BLOCK, BLOCK), BLOCK)
        cum = log_column(down, b)
        total = cum[BLOCK - 1 : BLOCK, :]
        span = tables.shape[1]
        for i in range(BLOCK // span):
            turn = angles((4 * sc[0] + sc[1]) * (tables.shape[1] // 16) + b * (BLOCK // span) + i, tables)
            here = pl.ds(pl.multiple_of(b * BLOCK + i * span, span), span)
            cosine[here, :], sine[here, :] = turn
        key = rotated(k[at, :].astype(f32), cosine[at, :], sine[at, :]) * k.shape[1] ** (-0.5)
        key = key.astype(bf16)
        kr[at, :] = key
        faded = (key.astype(f32) * jnp.exp(total - cum)).astype(bf16)
        add = lax.dot_general(faded, v[at, :], (((0,), (0,)), ((), ())), preferred_element_type=f32)
        prefix[b] = state[...].astype(bf16)
        state[...] = jnp.exp(total) * state[...] + add
        return 0

    lax.fori_loop(0, log.shape[1] // BLOCK, step, 0)
    everything = jnp.sum(log[...], axis=1, keepdims=True)
    tail = log_rows(everything, state.shape[1])
    rows = state.shape[0] // 4
    for d, out in enumerate((p0, p1, p2, p3)):
        at = pl.multiple_of(lax.rem(sc[1] + d, 4) * rows, rows)
        out[:rows] = state[pl.ds(at, rows), :].astype(bf16)
        out[rows:] = tail


def line_kernel(sc, r0, r1, r2, r3, total, entry, logs, pieces):
    rows = entry.shape[1]
    for d, r in enumerate((r0, r1, r2, r3)):
        pieces[lax.rem(sc[1] + 4 - d, 4)] = r[...]
    run = jnp.zeros(entry.shape[1:], f32)
    passed = jnp.zeros((1, 1), f32)
    for j in range(4):
        entry[j] = run
        logs[j : j + 1, :] = jnp.broadcast_to(passed, (1, logs.shape[1]))
        here = log_of(pieces[j, rows:].astype(f32))
        run = jnp.exp(here) * run + pieces[j, :rows].astype(f32)
        passed = passed + here
    total[:rows] = run.astype(bf16)
    total[rows:] = log_rows(passed, total.shape[1])


def incoming_kernel(sc, t1, t2, t3, entry, logs, o0, o1, o2, o3):
    rows = entry.shape[1]
    run = jnp.zeros(entry.shape[1:], f32)
    for d, t in ((3, t3), (2, t2), (1, t1)):
        new = jnp.exp(log_of(t[rows:].astype(f32))) * run + t[:rows].astype(f32)
        run = jnp.where(sc[0] >= d, new, run)
    for d, out in enumerate((o0, o1, o2, o3)):
        at = lax.rem(sc[1] + d, 4)
        fade = jnp.exp(logs[pl.ds(at, 1), 0:1])
        out[...] = (fade * run + entry[at]).astype(bf16)


def within_kernel(sc, down, across, kr, cosine, sine, prefix, q, v, within, scaled):
    lower = triangle(BLOCK)
    n = BLOCK // 4

    def step(b, _):
        at = pl.ds(pl.multiple_of(b * BLOCK, BLOCK), BLOCK)
        cum, row = log_column(down, b), log_row(across, b)
        query = rotated(q[at, :].astype(f32), cosine[at, :], sine[at, :]).astype(bf16)
        score = lax.dot_general(query, kr[at, :], (((1,), (1,)), ((), ())), preferred_element_type=f32)
        weight = jnp.where(lower, jnp.exp(jnp.where(lower, cum - row, 0.0)), 0.0)
        result = jnp.dot((score * weight).astype(bf16), v[at, :], preferred_element_type=f32)
        faded = (query.astype(f32) * jnp.exp(cum)).astype(bf16)
        result = result + jnp.dot(faded, prefix[b], preferred_element_type=f32)
        for i in range(4):
            to = pl.ds(pl.multiple_of((2 * b + i // 2) * n, n), n)
            within[i % 2, to, :] = result[i * n : (i + 1) * n]
            scaled[i % 2, to, :] = faded[i * n : (i + 1) * n]
        return 0

    lax.fori_loop(0, kr.shape[0] // BLOCK, step, 0)


def gated_kernel(sc, log, i0, i1, i2, i3, within, scaled, gate, out, start, carried, chunk):
    rows = i0.shape[0]
    for d, piece in enumerate((i0, i1, i2, i3)):
        at = pl.multiple_of(lax.rem(sc[1] + 4 - d, 4) * rows, rows)
        start[pl.ds(at, rows), :] = piece[...]
    order = lax.broadcasted_iota(jnp.int32, log.shape, 1)
    n = out.shape[0] // 8
    carried[...] = jnp.dot(scaled[chunk], start[...], preferred_element_type=f32)
    gated = []
    for b in range(log.shape[1] // BLOCK):
        passed = jnp.sum(jnp.where(order < b * BLOCK, log[...], 0.0), axis=1, keepdims=True)
        at = slice(2 * b * n, 2 * (b + 1) * n)
        mixed = within[chunk, at, :] + jnp.exp(passed) * carried[at, :]
        centred = mixed - jnp.mean(mixed, axis=1, keepdims=True)
        spread = jnp.mean(centred * centred, axis=1, keepdims=True)
        g = jnp.concatenate([gate[2 * b, chunk], gate[2 * b + 1, chunk]], axis=0).astype(f32)
        gated.append((g * jax.nn.sigmoid(g) * (centred * lax.rsqrt(spread + EPS))).astype(bf16))
    out[...] = jnp.concatenate(gated, axis=0)


def heads_project_kernel(sc, gated, weight, keep, send):
    place(keep, send, sc, sc[3] == 0, lambda cols: jnp.dot(gated[...], weight[:, cols], preferred_element_type=f32))


def heads_kernel(sc, log, i0, i1, i2, i3, within, scaled, gate, weight, keep, send, start, carried, gated, chunk):
    gated_kernel(sc, log, i0, i1, i2, i3, within, scaled, gate, gated, start, carried, chunk)
    heads_project_kernel(sc, gated, weight, keep, send)


def place(keep, send, sc, south, product, tile=512):
    n = keep.shape[1]
    for j in range(keep.shape[2] // tile):
        cols = slice(j * tile, (j + 1) * tile)
        part = product(cols).astype(bf16)
        for xx in range(4):
            lo, hi = part[2 * xx * n : (2 * xx + 1) * n], part[(2 * xx + 1) * n : (2 * xx + 2) * n]
            at = lax.rem(xx + 4 - sc[2], 4)
            keep[at, :, cols] = jnp.where(south, lo, hi)
            send[at, :, cols] = jnp.where(south, hi, lo)


def scatter_kernel(sc, keep, got, s1, s2, s3):
    for d, out in ((1, s1), (2, s2), (3, s3)):
        out[...] = (keep[d].astype(f32) + got[d].astype(f32)).astype(bf16)


def norm_kernel(sc, keep, got, r1, r2, r3, base, gain, shift, *rest, row, group):
    out, rows = rest[0], keep.shape[1]
    total = keep[0].astype(f32) + got[0].astype(f32) + r1[...].astype(f32)
    total = total + r2[...].astype(f32) + r3[...].astype(f32)
    at = 0 if group is None else 4 * sc[2] + 2 * sc[3] + group
    total = total + ALPHA * base[at].astype(f32)
    centred = total - jnp.mean(total, axis=1, keepdims=True)
    spread = jnp.mean(centred * centred, axis=1, keepdims=True)
    if len(rest) > 1:
        after, target, own, sems = rest
        later = pltpu.make_async_copy(after, target.at[pl.ds(rows, after.shape[0])], sems.at[1])
        later.start()
    result = (
        centred * lax.rsqrt(spread + EPS) * gain[row : row + 1, :] + shift[row : row + 1, :]
    ).astype(bf16)
    if len(rest) == 1:
        out[...] = result
        return
    own[...] = result
    mine = pltpu.make_async_copy(own, target.at[pl.ds(0, rows)], sems.at[0])
    mine.start()
    mine.wait()
    later.wait()


def reduce_and_norm(sc, keep, send, base, gain, shift, row, group, *after):
    _, rows, width = keep.shape
    piece = ((rows, width), bf16)
    got = swap_cores(send)
    size = rows * width
    sums = run(scatter_kernel, sc, (keep, got), [piece] * 3, flops=size * 400)
    far = [shift_by(s, "x", d) for d, s in zip((1, 2, 3), sums)]
    return run(
        functools.partial(norm_kernel, row=row, group=group),
        sc, (keep, got, *far, base, gain, shift, *after), [((rows * (1 + len(after)), width), bf16)], flops=size * 400,
        far_outs=len(after), scratch=[pltpu.VMEM(*piece), pltpu.SemaphoreType.DMA((2,))] if after else [],
    )[0]


def gather_rows(own):
    mine = everyone(own, "x")
    return mine + [swap_cores(m) for m in mine]


def opening_kernel(sc, *refs):
    sources, gate, value, down = refs[:5], *refs[5:8]
    homes, shard = refs[8:13], refs[13]
    gate_v, value_v, down_v, both, sems, weight_sems = refs[14:]
    loads = [
        pltpu.make_async_copy(src, dst, weight_sems.at[i])
        for i, (src, dst) in enumerate(((gate, gate_v), (value, value_v), (down, down_v)))
    ]
    moves = [pltpu.make_async_copy(src, dst, sems.at[i]) for i, (src, dst) in enumerate(zip(sources, homes))]
    for copy in loads + moves:
        copy.start()
    for copy in loads:
        copy.wait()
    parts = [r[...] for r in (gate_v, value_v, down_v)]
    rest = both.shape[1] - sum(p.shape[0] for p in parts)
    both[...] = jnp.concatenate(parts + [jnp.zeros((rest, both.shape[0]), bf16)], axis=0).T
    out = pltpu.make_async_copy(both, shard, weight_sems.at[3])
    out.start()
    for copy in moves:
        copy.wait()
    out.wait()


def gather_into(sc, pieces, rows):
    n = pieces[0].shape[0]
    for i, piece in enumerate(pieces):
        core = sc[3] if i < 4 else 1 - sc[3]
        at = pl.multiple_of((2 * lax.rem(sc[2] + 4 - i % 4, 4) + core) * n, n)
        rows[pl.ds(at, n), :] = piece[...]


def first_up_kernel(sc, *refs):
    pieces, weight, out, up, down, rows, total, sems = refs[:8], *refs[8:]
    steps = sems.shape[0] - 1
    deep = up.shape[0] // steps
    parts = [slice(i * deep, (i + 1) * deep) for i in range(steps)]
    loads = [
        pltpu.make_async_copy(weight.at[p, pl.ds(0, up.shape[1])], up.at[p], sems.at[i]) for i, p in enumerate(parts)
    ]
    loads.append(pltpu.make_async_copy(weight.at[:, pl.ds(up.shape[1], down.shape[1])], down, sems.at[steps]))
    for load in loads:
        load.start()
    gather_into(sc, pieces, rows)
    for i, p in enumerate(parts):
        loads[i].wait()
        part = jnp.dot(rows[:, p], up[p, :], preferred_element_type=f32)
        if i == 0:
            total[...] = part
        elif i < steps - 1:
            total[...] += part
        else:
            out[...] = (total[...] + part).astype(bf16)
    loads[steps].wait()


def second_up_kernel(sc, *refs):
    pieces, weight, out, rows = refs[:8], *refs[8:]
    gather_into(sc, pieces, rows)
    out[...] = jnp.dot(rows[...], weight[...], preferred_element_type=f32).astype(bf16)


def first_up(sc, pieces, weights, hidden):
    n, width = pieces[0].shape
    return run(
        first_up_kernel, sc, (*pieces, weights),
        [((8 * n, hidden), bf16), ((width, hidden), bf16), ((width, weights.shape[1] - hidden), bf16)],
        scratch=[
            pltpu.VMEM((8 * n, width), bf16), pltpu.VMEM((8 * n, hidden), f32), pltpu.SemaphoreType.DMA((5,))
        ],
        flops=16 * n * width * hidden, limit=16, far=1,
    )


def second_up(sc, pieces, weights, hidden):
    n, width = pieces[0].shape
    return run(
        second_up_kernel, sc, (*pieces, weights), [((8 * n, hidden), bf16)],
        scratch=[pltpu.VMEM((8 * n, width), bf16)], flops=16 * n * width * hidden, limit=16,
    )[0]


def activate_kernel(sc, mine, other, edge, taps, bias, active, chunk):
    n = mine.shape[0] // 8
    hidden = active.shape[1]

    def conv_group(t, _):
        at = pl.multiple_of(t * n, n)
        if chunk == 1:
            halo = other[pl.ds(pl.multiple_of(at + n - 16, 16), 16), :][8:]
        else:
            before = pl.multiple_of(jnp.maximum(at - 16, 0), 16)
            halo = jnp.where(t == 0, edge[8:].astype(f32), other[pl.ds(before, 16), :][8:].astype(f32))
        rows = jnp.concatenate([halo.astype(f32), mine[pl.ds(at, n), :].astype(f32)], axis=0)
        conv = bias[0:1, :] + pltpu.roll(rows, 2, 0)[8:] * taps[0:1, :]
        conv = conv + pltpu.roll(rows, 1, 0)[8:] * taps[1:2, :]
        conv = conv + rows[8:] * taps[2:3, :]
        active[pl.ds(at, n), :] = (jax.nn.gelu(conv[:, :hidden]) * conv[:, hidden:]).astype(bf16)
        return 0

    lax.fori_loop(0, 8, conv_group, 0)


def project_kernel(sc, active, weight, keep, send):
    hidden = active.shape[1]
    place(keep, send, sc, sc[3] == 0, lambda cols: lax.dot_general(
        active[...], weight[cols, :hidden], (((1,), (1,)), ((), ())), preferred_element_type=f32
    ))


def down_kernel(sc, mine, other, edge, taps, bias, weight, keep, send, active, chunk):
    activate_kernel(sc, mine, other, edge, taps, bias, active, chunk)
    project_kernel(sc, active, weight, keep, send)


def down_project(sc, mine, other, edge, taps, bias, weights, width, chunk):
    rows, double = mine.shape
    n = rows // 8
    shape = ((4, n, width), bf16)
    hidden = ((rows, double // 2), bf16)
    if chunk == 0:
        sources = (mine, other, edge, taps, bias)
        active = run(
            functools.partial(activate_kernel, chunk=chunk), sc, sources, [hidden], flops=rows * width * double
        )[0]
        return run(project_kernel, sc, (active, weights), [shape, shape], flops=rows * width * double)
    return run(
        functools.partial(down_kernel, chunk=chunk), sc,
        (mine, other, edge, taps, bias, weights), [shape, shape],
        scratch=[pltpu.VMEM((rows, double // 2), bf16)],
        flops=rows * width * double * 2, limit=16,
    )


def shards(
    query_proj, key_proj, value_proj, gate_proj, log_decay, residual, out_weight, norm_gain,
    norm_bias, up_gate, up_value, conv_weight, conv_bias, down_weight,
):
    tok, dk = query_proj.shape
    dv = value_proj.shape[1]
    width = residual.shape[1]
    hidden = up_gate.shape[1]
    blocks = tok // BLOCK
    n = tok // 16
    taps = jnp.concatenate([conv_weight[0], conv_weight[1]], axis=1)
    bias = jnp.concatenate([conv_bias[0:1], conv_bias[1:2]], axis=1)
    sc = jnp.stack([lax.axis_index(a) for a in ("z", "y", "x", "c")]).astype(jnp.int32)

    tables = jnp.asarray(trig_tables(dk // 2, 128, 128))
    padded = -(-3 * hidden // 128) * 128
    near = (log_decay.T, query_proj, key_proj, value_proj, tables)
    column = ((hidden, up_gate.shape[0]), bf16)
    log, query, key, value, tables, shard = run(
        opening_kernel, sc, (*near, up_gate.T, up_value.T, down_weight),
        [(a.shape, a.dtype) for a in near] + [((up_gate.shape[0], padded), bf16)],
        scratch=[pltpu.VMEM(*column)] * 3
        + [pltpu.VMEM((up_gate.shape[0], padded), bf16), pltpu.SemaphoreType.DMA((5,)), pltpu.SemaphoreType.DMA((4,))],
        flops=1 << 26, far=8, far_outs=1,
    )
    weights = lax.all_gather(shard, SP, axis=0, tiled=True)
    piece = ((dk // 4 + EXTRA, dv), bf16)
    turn = ((tok, dk // 2), f32)
    key_rot, cosine, sine, prefix, down_logs, across_logs, *pieces = run(
        states_kernel, sc, (log, key, value, tables),
        [((tok, dk), bf16), turn, turn, ((blocks, dk, dv), bf16), ((BLOCK, 4 * blocks), f32), ((4 * blocks, BLOCK), f32)]
        + [piece] * 4,
        scratch=[pltpu.VMEM((dk, dv), f32)], flops=4 * tok * dk * dv,
    )
    got = [pieces[0]] + [shift_by(pieces[d], "y", d) for d in (1, 2, 3)]
    within, scaled = run(
        within_kernel, sc, (down_logs, across_logs, key_rot, cosine, sine, prefix, query, value),
        [((2, tok // 2, dv), f32), ((2, tok // 2, dk), bf16)],
        flops=4 * tok * BLOCK * (dk + dv),
    )
    total, entry, logs = run(
        line_kernel, sc, got, [piece, ((4, dk // 4, dv), f32), ((8, 128), f32)],
        scratch=[pltpu.VMEM((4,) + piece[0], bf16)], flops=100 * dk * dv,
    )
    lines = everyone(total, "z")[1:]
    quarter = ((dk // 4, dv), bf16)
    outgoing = run(incoming_kernel, sc, (*lines, entry, logs), [quarter] * 4, flops=100 * dk * dv)
    incoming = [outgoing[0]] + [shift_by(outgoing[d], "y", d) for d in (1, 2, 3)]
    gates = gate_proj.reshape(8, 2, n, dv)
    bases = residual.reshape(16, n, width)
    normed, ups, rows = [None, None], [None, None], [None, None]
    for k in (1, 0):
        shape = ((4, n, width), bf16)
        sources = (log, *incoming, within, scaled, gates)
        scratch = [pltpu.VMEM((dk, dv), bf16), pltpu.VMEM((tok // 2, dv), f32)]
        gated = ((tok // 2, dv), bf16)
        if k == 0:
            ready = run(
                functools.partial(gated_kernel, chunk=k), sc, sources, [gated],
                scratch=scratch, flops=tok * dv * dk,
            )[0]
            keep, send = run(heads_project_kernel, sc, (ready, out_weight), [shape, shape], flops=tok * dv * width)
        else:
            keep, send = run(
                functools.partial(heads_kernel, chunk=k), sc, (*sources, out_weight), [shape, shape],
                scratch=scratch + [pltpu.VMEM(*gated)], flops=tok * dv * (dk + width),
            )
        normed[k] = reduce_and_norm(sc, keep, send, bases, norm_gain, norm_bias, 0, k)
        rows[k] = gather_rows(normed[k])
    ups[1], weights, down_weights = first_up(sc, rows[1], weights, 2 * hidden)
    ups[0] = second_up(sc, rows[0], weights, 2 * hidden)
    edge = lax.ppermute(ups[1][8 * n - 16 :], SP, [(i, i + 1) for i in range(15)])
    outs = [None, None]
    for k in (1, 0):
        keep, send = down_project(sc, ups[k], ups[1 - k], edge, taps, bias, down_weights, width, k)
        outs[k] = reduce_and_norm(sc, keep, send, normed[k][None], norm_gain, norm_bias, 1, None, *outs[k + 1 :])
    return outs[0]


def solution(mesh):
    torus = Mesh(mesh.devices.reshape(4, 4, 4, 2), SP + TP)
    return jax.shard_map(
        shards,
        mesh=torus,
        in_specs=(
            P(SP, TP),
            P(SP, TP),
            P(SP, TP),
            P(SP, TP),
            P(SP, TP),
            P(SP, None),
            P(TP, None),
            P(),
            P(),
            P(SP, TP),
            P(SP, TP),
            P(None, None, TP),
            P(None, TP),
            P(TP, SP),
        ),
        out_specs=P(SP + TP, None),
        check_vma=False,
    )
```

```python
import functools

import jax
import jax.numpy as jnp
import numpy as np
from jax import lax
from jax.experimental import pallas as pl
from jax.experimental.pallas import tpu as pltpu
from jax.sharding import Mesh
from jax.sharding import PartitionSpec as P


BLOCK = 256
SP = ("z", "y")
TP = ("x", "c")
f32 = jnp.float32
bf16 = jnp.bfloat16

ALPHA = 8.0**0.25
ROPE_BASE = 10000.0
EPS = 1e-05
EXTRA = 16


def ring(shift, size=4):
    return [(i, (i + shift) % size) for i in range(size)]


def shift_by(x, axis, by):
    return lax.ppermute(x, axis, ring(by))


def everyone(x, axis):
    return [x] + [shift_by(x, axis, d) for d in (1, 2, 3)]


def swap_cores(x):
    return lax.ppermute(x, "c", [(0, 1), (1, 0)])


def run(kernel, sc, args, outs, scratch=(), flops=0, limit=8, far=0, far_outs=0):
    near, away = pl.BlockSpec(memory_space=pltpu.VMEM), pl.BlockSpec(memory_space=pltpu.HBM)
    split, kept = len(args) - far, len(outs) - far_outs
    args = [pltpu.with_memory_space_constraint(a, pltpu.VMEM if i < split else pltpu.HBM) for i, a in enumerate(args)]
    spaces = [pltpu.VMEM] * kept + [pltpu.HBM] * far_outs
    return pl.pallas_call(
        kernel,
        in_specs=[pl.BlockSpec(memory_space=pltpu.SMEM)] + [near] * split + [away] * far,
        out_specs=[near] * kept + [away] * far_outs,
        out_shape=[space(shape, dtype) for space, (shape, dtype) in zip(spaces, outs)],
        scratch_shapes=scratch,
        cost_estimate=pl.CostEstimate(flops=flops, transcendentals=0, bytes_accessed=0),
        compiler_params=pltpu.CompilerParams(vmem_limit_bytes=limit << 20),
    )(sc, *args)


def trig_tables(half, rows, count):
    freq = ROPE_BASE ** (-2.0 * np.arange(half, dtype=np.float64) / (2 * half))
    low = np.arange(rows, dtype=np.float64)[:, None] * freq[None, :]
    high = rows * np.arange(count, dtype=np.float64)[:, None] * freq[None, :]
    return np.stack([np.cos(low), np.sin(low), np.cos(high), np.sin(high)]).astype(np.float32)


def angles(at, tables):
    high_cos, high_sin = tables[2, pl.ds(at, 1), :], tables[3, pl.ds(at, 1), :]
    cos = high_cos * tables[0] - high_sin * tables[1]
    return cos, high_sin * tables[0] + high_cos * tables[1]


def rotated(x, cos, sin):
    half = cos.shape[1]
    front, second = x[:, :half], x[:, half:]
    return jnp.concatenate([front * cos - second * sin, front * sin + second * cos], axis=1)


def triangle(n):
    r = lax.broadcasted_iota(jnp.int32, (n, n), 0)
    c = lax.broadcasted_iota(jnp.int32, (n, n), 1)
    return r >= c


def split_logs(log):
    blocks = log.shape[1] // BLOCK
    whole = jnp.concatenate([log[:, b * BLOCK : (b + 1) * BLOCK] for b in range(blocks)], axis=0)
    first = whole.astype(bf16).astype(f32)
    second = (whole - first).astype(bf16).astype(f32)
    third = whole - first - second
    return jnp.concatenate([first, second, third, jnp.zeros_like(whole)], axis=0).astype(bf16)


def running_logs(log, down, across):
    terms = split_logs(log[...])
    lower = triangle(BLOCK).astype(f32).astype(bf16)
    last = (((1,), (1,)), ((), ()))
    down[...] = lax.dot_general(lower, terms, last, preferred_element_type=f32)
    across[...] = lax.dot_general(terms, lower, last, preferred_element_type=f32)


def log_column(down, b):
    lane = lax.broadcasted_iota(jnp.int32, down.shape, 1)
    blocks = down.shape[1] // 4
    mine = (lane == b) | (lane == b + blocks) | (lane == b + 2 * blocks)
    return jnp.sum(jnp.where(mine, down[...], 0.0), axis=1, keepdims=True)


def log_row(across, b):
    blocks = across.shape[0] // 4
    return across[pl.ds(b, 1), :] + across[pl.ds(b + blocks, 1), :] + across[pl.ds(b + 2 * blocks, 1), :]


def log_rows(total, width):
    a = total.astype(bf16)
    b = (total - a.astype(f32)).astype(bf16)
    c = (total - a.astype(f32) - b.astype(f32)).astype(bf16)
    at = lax.broadcasted_iota(jnp.int32, (EXTRA, width), 0)
    pick = jnp.where(at == 0, a.astype(f32), jnp.where(at == 1, b.astype(f32), c.astype(f32)))
    return jnp.where(at < 3, pick, 0.0).astype(bf16)


def log_of(rows):
    return rows[0:1, 0:1] + rows[1:2, 0:1] + rows[2:3, 0:1]


def states_kernel(sc, log, k, v, tables, kr, cosine, sine, prefix, down, across, p0, p1, p2, p3, state):
    running_logs(log, down, across)
    state[...] = jnp.zeros_like(state)

    def step(b, _):
        at = pl.ds(pl.multiple_of(b * BLOCK, BLOCK), BLOCK)
        cum = log_column(down, b)
        total = cum[BLOCK - 1 : BLOCK, :]
        span = tables.shape[1]
        for i in range(BLOCK // span):
            turn = angles((4 * sc[0] + sc[1]) * (tables.shape[1] // 16) + b * (BLOCK // span) + i, tables)
            here = pl.ds(pl.multiple_of(b * BLOCK + i * span, span), span)
            cosine[here, :], sine[here, :] = turn
        key = rotated(k[at, :].astype(f32), cosine[at, :], sine[at, :]) * k.shape[1] ** (-0.5)
        key = key.astype(bf16)
        kr[at, :] = key
        faded = (key.astype(f32) * jnp.exp(total - cum)).astype(bf16)
        add = lax.dot_general(faded, v[at, :], (((0,), (0,)), ((), ())), preferred_element_type=f32)
        prefix[b] = state[...].astype(bf16)
        state[...] = jnp.exp(total) * state[...] + add
        return 0

    lax.fori_loop(0, log.shape[1] // BLOCK, step, 0)
    everything = jnp.sum(log[...], axis=1, keepdims=True)
    tail = log_rows(everything, state.shape[1])
    rows = state.shape[0] // 4
    for d, out in enumerate((p0, p1, p2, p3)):
        at = pl.multiple_of(lax.rem(sc[1] + d, 4) * rows, rows)
        out[:rows] = state[pl.ds(at, rows), :].astype(bf16)
        out[rows:] = tail


def line_kernel(sc, r0, r1, r2, r3, total, entry, logs, pieces):
    rows = entry.shape[1]
    for d, r in enumerate((r0, r1, r2, r3)):
        pieces[lax.rem(sc[1] + 4 - d, 4)] = r[...]
    run = jnp.zeros(entry.shape[1:], f32)
    passed = jnp.zeros((1, 1), f32)
    for j in range(4):
        entry[j] = run
        logs[j : j + 1, :] = jnp.broadcast_to(passed, (1, logs.shape[1]))
        here = log_of(pieces[j, rows:].astype(f32))
        run = jnp.exp(here) * run + pieces[j, :rows].astype(f32)
        passed = passed + here
    total[:rows] = run.astype(bf16)
    total[rows:] = log_rows(passed, total.shape[1])


def incoming_kernel(sc, t1, t2, t3, entry, logs, o0, o1, o2, o3):
    rows = entry.shape[1]
    run = jnp.zeros(entry.shape[1:], f32)
    for d, t in ((3, t3), (2, t2), (1, t1)):
        new = jnp.exp(log_of(t[rows:].astype(f32))) * run + t[:rows].astype(f32)
        run = jnp.where(sc[0] >= d, new, run)
    for d, out in enumerate((o0, o1, o2, o3)):
        at = lax.rem(sc[1] + d, 4)
        fade = jnp.exp(logs[pl.ds(at, 1), 0:1])
        out[...] = (fade * run + entry[at]).astype(bf16)


def within_kernel(sc, down, across, kr, cosine, sine, prefix, q, v, within, scaled):
    lower = triangle(BLOCK)
    n = BLOCK // 4

    def step(b, _):
        at = pl.ds(pl.multiple_of(b * BLOCK, BLOCK), BLOCK)
        cum, row = log_column(down, b), log_row(across, b)
        query = rotated(q[at, :].astype(f32), cosine[at, :], sine[at, :]).astype(bf16)
        score = lax.dot_general(query, kr[at, :], (((1,), (1,)), ((), ())), preferred_element_type=f32)
        weight = jnp.where(lower, jnp.exp(jnp.where(lower, cum - row, 0.0)), 0.0)
        result = jnp.dot((score * weight).astype(bf16), v[at, :], preferred_element_type=f32)
        faded = (query.astype(f32) * jnp.exp(cum)).astype(bf16)
        result = result + jnp.dot(faded, prefix[b], preferred_element_type=f32)
        for i in range(4):
            to = pl.ds(pl.multiple_of((2 * b + i // 2) * n, n), n)
            within[i % 2, to, :] = result[i * n : (i + 1) * n]
            scaled[i % 2, to, :] = faded[i * n : (i + 1) * n]
        return 0

    lax.fori_loop(0, kr.shape[0] // BLOCK, step, 0)


def gated_kernel(sc, log, i0, i1, i2, i3, within, scaled, gate, out, start, carried, chunk):
    rows = i0.shape[0]
    for d, piece in enumerate((i0, i1, i2, i3)):
        at = pl.multiple_of(lax.rem(sc[1] + 4 - d, 4) * rows, rows)
        start[pl.ds(at, rows), :] = piece[...]
    order = lax.broadcasted_iota(jnp.int32, log.shape, 1)
    n = out.shape[0] // 8
    carried[...] = jnp.dot(scaled[chunk], start[...], preferred_element_type=f32)
    gated = []
    for b in range(log.shape[1] // BLOCK):
        passed = jnp.sum(jnp.where(order < b * BLOCK, log[...], 0.0), axis=1, keepdims=True)
        at = slice(2 * b * n, 2 * (b + 1) * n)
        mixed = within[chunk, at, :] + jnp.exp(passed) * carried[at, :]
        centred = mixed - jnp.mean(mixed, axis=1, keepdims=True)
        spread = jnp.mean(centred * centred, axis=1, keepdims=True)
        g = jnp.concatenate([gate[2 * b, chunk], gate[2 * b + 1, chunk]], axis=0).astype(f32)
        gated.append((g * jax.nn.sigmoid(g) * (centred * lax.rsqrt(spread + EPS))).astype(bf16))
    out[...] = jnp.concatenate(gated, axis=0)


def project(out, sc, own, active, product, tile=256):
    n = out.shape[1]
    core = sc[3] if own else 1 - sc[3]
    rows = [active[pl.ds(pl.multiple_of((2 * chip + core) * n, n), n), :] for chip in range(4)]
    rows = jnp.concatenate(rows, axis=0)
    for j in range(out.shape[2] // tile):
        cols = slice(j * tile, (j + 1) * tile)
        part = product(rows, cols).astype(bf16)
        for chip in range(4):
            out[lax.rem(chip + 4 - sc[2], 4), :, cols] = part[chip * n : (chip + 1) * n]


def heads_project_kernel(sc, gated, weight, out, own):
    project(out, sc, own, gated, lambda rows, cols: jnp.dot(rows, weight[:, cols], preferred_element_type=f32))


def heads_kernel(sc, log, i0, i1, i2, i3, within, scaled, gate, weight, gated, send, start, carried, chunk):
    gated_kernel(sc, log, i0, i1, i2, i3, within, scaled, gate, gated, start, carried, chunk)
    heads_project_kernel(sc, gated, weight, send, False)


def place(keep, send, sc, south, product, tile=256):
    n = keep.shape[1]
    for j in range(keep.shape[2] // tile):
        cols = slice(j * tile, (j + 1) * tile)
        part = product(cols).astype(bf16)
        for xx in range(4):
            lo, hi = part[2 * xx * n : (2 * xx + 1) * n], part[(2 * xx + 1) * n : (2 * xx + 2) * n]
            at = lax.rem(xx + 4 - sc[2], 4)
            keep[at, :, cols] = jnp.where(south, lo, hi)
            send[at, :, cols] = jnp.where(south, hi, lo)


def scatter_kernel(sc, keep, got, s1, s2, s3):
    for d, out in ((1, s1), (2, s2), (3, s3)):
        out[...] = (keep[d].astype(f32) + got[d].astype(f32)).astype(bf16)


def norm_kernel(sc, keep, got, r1, r2, r3, base, gain, shift, *rest, row, group):
    out, rows = rest[0], keep.shape[1]
    total = keep[0].astype(f32) + got[0].astype(f32) + r1[...].astype(f32)
    total = total + r2[...].astype(f32) + r3[...].astype(f32)
    at = 0 if group is None else 4 * sc[2] + 2 * sc[3] + group
    total = total + ALPHA * base[at].astype(f32)
    centred = total - jnp.mean(total, axis=1, keepdims=True)
    spread = jnp.mean(centred * centred, axis=1, keepdims=True)
    if len(rest) > 1:
        after, target, own, sems = rest
        later = pltpu.make_async_copy(after, target.at[pl.ds(rows, after.shape[0])], sems.at[1])
        later.start()
    result = (
        centred * lax.rsqrt(spread + EPS) * gain[row : row + 1, :] + shift[row : row + 1, :]
    ).astype(bf16)
    if len(rest) == 1:
        out[...] = result
        return
    own[...] = result
    mine = pltpu.make_async_copy(own, target.at[pl.ds(0, rows)], sems.at[0])
    mine.start()
    mine.wait()
    later.wait()


def reduce_and_norm(sc, keep, send, base, gain, shift, row, group, *after):
    _, rows, width = keep.shape
    piece = ((rows, width), bf16)
    got = swap_cores(send)
    size = rows * width
    sums = run(scatter_kernel, sc, (keep, got), [piece] * 3, flops=size * 400)
    far = [shift_by(s, "x", d) for d, s in zip((1, 2, 3), sums)]
    return run(
        functools.partial(norm_kernel, row=row, group=group),
        sc, (keep, got, *far, base, gain, shift, *after), [((rows * (1 + len(after)), width), bf16)], flops=size * 400,
        far_outs=len(after), scratch=[pltpu.VMEM(*piece), pltpu.SemaphoreType.DMA((2,))] if after else [],
    )[0]


def gather_rows(own):
    mine = everyone(own, "x")
    return mine + [swap_cores(m) for m in mine]


def opening_kernel(sc, *refs):
    sources, gate, value, down = refs[:4], *refs[4:7]
    homes, shard = refs[7:11], refs[11]
    gate_v, value_v, down_v, both, sems, weight_sems = refs[12:]
    loads = [
        pltpu.make_async_copy(src, dst, weight_sems.at[i])
        for i, (src, dst) in enumerate(((gate, gate_v), (value, value_v), (down, down_v)))
    ]
    moves = [pltpu.make_async_copy(src, dst, sems.at[i]) for i, (src, dst) in enumerate(zip(sources, homes))]
    for copy in loads + moves:
        copy.start()
    for copy in loads:
        copy.wait()
    parts = [r[...] for r in (gate_v, value_v, down_v)]
    rest = both.shape[1] - sum(p.shape[0] for p in parts)
    both[...] = jnp.concatenate(parts + [jnp.zeros((rest, both.shape[0]), bf16)], axis=0).T
    out = pltpu.make_async_copy(both, shard, weight_sems.at[3])
    out.start()
    for copy in moves:
        copy.wait()
    out.wait()


def gather_into(sc, pieces, rows):
    n = pieces[0].shape[0]
    for i, piece in enumerate(pieces):
        core = sc[3] if i < 4 else 1 - sc[3]
        at = pl.multiple_of((2 * lax.rem(sc[2] + 4 - i % 4, 4) + core) * n, n)
        rows[pl.ds(at, n), :] = piece[...]


def first_up_kernel(sc, *refs):
    pieces, weight, out, up, down, rows, total, sems = refs[:8], *refs[8:]
    steps = sems.shape[0] - 1
    deep = up.shape[0] // steps
    parts = [slice(i * deep, (i + 1) * deep) for i in range(steps)]
    loads = [
        pltpu.make_async_copy(weight.at[p, pl.ds(0, up.shape[1])], up.at[p], sems.at[i]) for i, p in enumerate(parts)
    ]
    loads.append(pltpu.make_async_copy(weight.at[:, pl.ds(up.shape[1], down.shape[1])], down, sems.at[steps]))
    for load in loads:
        load.start()
    gather_into(sc, pieces, rows)
    for i, p in enumerate(parts):
        loads[i].wait()
        part = jnp.dot(rows[:, p], up[p, :], preferred_element_type=f32)
        if i == 0:
            total[...] = part
        elif i < steps - 1:
            total[...] += part
        else:
            out[...] = (total[...] + part).astype(bf16)
    loads[steps].wait()


def second_up_kernel(sc, *refs):
    pieces, weight, out, rows = refs[:8], *refs[8:]
    gather_into(sc, pieces, rows)
    out[...] = jnp.dot(rows[...], weight[...], preferred_element_type=f32).astype(bf16)


def first_up(sc, pieces, weights, hidden):
    n, width = pieces[0].shape
    return run(
        first_up_kernel, sc, (*pieces, weights),
        [((8 * n, hidden), bf16), ((width, hidden), bf16), ((width, weights.shape[1] - hidden), bf16)],
        scratch=[
            pltpu.VMEM((8 * n, width), bf16), pltpu.VMEM((8 * n, hidden), f32), pltpu.SemaphoreType.DMA((5,))
        ],
        flops=16 * n * width * hidden, limit=16, far=1,
    )


def second_up(sc, pieces, weights, hidden):
    n, width = pieces[0].shape
    return run(
        second_up_kernel, sc, (*pieces, weights), [((8 * n, hidden), bf16)],
        scratch=[pltpu.VMEM((8 * n, width), bf16)], flops=16 * n * width * hidden, limit=16,
    )[0]


def activate_kernel(sc, mine, other, edge, taps, bias, active, chunk):
    n = mine.shape[0] // 8
    hidden = active.shape[1]

    def conv_group(t, _):
        at = pl.multiple_of(t * n, n)
        if chunk == 1:
            halo = other[pl.ds(pl.multiple_of(at + n - 16, 16), 16), :][8:]
        else:
            before = pl.multiple_of(jnp.maximum(at - 16, 0), 16)
            halo = jnp.where(t == 0, edge[8:].astype(f32), other[pl.ds(before, 16), :][8:].astype(f32))
        rows = jnp.concatenate([halo.astype(f32), mine[pl.ds(at, n), :].astype(f32)], axis=0)
        conv = bias[0:1, :] + pltpu.roll(rows, 2, 0)[8:] * taps[0:1, :]
        conv = conv + pltpu.roll(rows, 1, 0)[8:] * taps[1:2, :]
        conv = conv + rows[8:] * taps[2:3, :]
        active[pl.ds(at, n), :] = (jax.nn.gelu(conv[:, :hidden]) * conv[:, hidden:]).astype(bf16)
        return 0

    lax.fori_loop(0, 8, conv_group, 0)


def project_kernel(sc, active, weight, keep, send):
    hidden = active.shape[1]
    place(keep, send, sc, sc[3] == 0, lambda cols: lax.dot_general(
        active[...], weight[cols, :hidden], (((1,), (1,)), ((), ())), preferred_element_type=f32
    ))


def down_kernel(sc, mine, other, edge, taps, bias, weight, keep, send, active, chunk):
    activate_kernel(sc, mine, other, edge, taps, bias, active, chunk)
    project_kernel(sc, active, weight, keep, send)


def down_project(sc, mine, other, edge, taps, bias, weights, width, chunk):
    rows, double = mine.shape
    n = rows // 8
    shape = ((4, n, width), bf16)
    hidden = ((rows, double // 2), bf16)
    if chunk == 0:
        sources = (mine, other, edge, taps, bias)
        active = run(
            functools.partial(activate_kernel, chunk=chunk), sc, sources, [hidden], flops=rows * width * double
        )[0]
        return run(project_kernel, sc, (active, weights), [shape, shape], flops=rows * width * double)
    return run(
        functools.partial(down_kernel, chunk=chunk), sc,
        (mine, other, edge, taps, bias, weights), [shape, shape],
        scratch=[pltpu.VMEM((rows, double // 2), bf16)],
        flops=rows * width * double * 2, limit=16,
    )


def shards(
    query_proj, key_proj, value_proj, gate_proj, log_decay, residual, out_weight, norm_gain,
    norm_bias, up_gate, up_value, conv_weight, conv_bias, down_weight,
):
    tok, dk = query_proj.shape
    dv = value_proj.shape[1]
    width = residual.shape[1]
    hidden = up_gate.shape[1]
    blocks = tok // BLOCK
    n = tok // 16
    taps = jnp.concatenate([conv_weight[0], conv_weight[1]], axis=1)
    bias = jnp.concatenate([conv_bias[0:1], conv_bias[1:2]], axis=1)
    sc = jnp.stack([lax.axis_index(a) for a in ("z", "y", "x", "c")]).astype(jnp.int32)

    tables = jnp.asarray(trig_tables(dk // 2, 128, 128))
    padded = -(-3 * hidden // 128) * 128
    near = (log_decay.T, key_proj, value_proj, tables)
    column = ((hidden, up_gate.shape[0]), bf16)
    log, key, value, tables, shard = run(
        opening_kernel, sc, (*near, up_gate.T, up_value.T, down_weight),
        [(a.shape, a.dtype) for a in near] + [((up_gate.shape[0], padded), bf16)],
        scratch=[pltpu.VMEM(*column)] * 3
        + [pltpu.VMEM((up_gate.shape[0], padded), bf16), pltpu.SemaphoreType.DMA((4,)), pltpu.SemaphoreType.DMA((4,))],
        flops=1 << 26, far=7, far_outs=1,
    )
    weights = lax.all_gather(shard, SP, axis=0, tiled=True)
    piece = ((dk // 4 + EXTRA, dv), bf16)
    turn = ((tok, dk // 2), f32)
    key_rot, cosine, sine, prefix, down_logs, across_logs, *pieces = run(
        states_kernel, sc, (log, key, value, tables),
        [((tok, dk), bf16), turn, turn, ((blocks, dk, dv), bf16), ((BLOCK, 4 * blocks), f32), ((4 * blocks, BLOCK), f32)]
        + [piece] * 4,
        scratch=[pltpu.VMEM((dk, dv), f32)], flops=4 * tok * dk * dv,
    )
    got = [pieces[0]] + [shift_by(pieces[d], "y", d) for d in (1, 2, 3)]
    within, scaled = run(
        within_kernel, sc, (down_logs, across_logs, key_rot, cosine, sine, prefix, query_proj, value),
        [((2, tok // 2, dv), f32), ((2, tok // 2, dk), bf16)],
        flops=4 * tok * BLOCK * (dk + dv),
    )
    total, entry, logs = run(
        line_kernel, sc, got, [piece, ((4, dk // 4, dv), f32), ((8, 128), f32)],
        scratch=[pltpu.VMEM((4,) + piece[0], bf16)], flops=100 * dk * dv,
    )
    lines = everyone(total, "z")[1:]
    quarter = ((dk // 4, dv), bf16)
    outgoing = run(incoming_kernel, sc, (*lines, entry, logs), [quarter] * 4, flops=100 * dk * dv)
    incoming = [outgoing[0]] + [shift_by(outgoing[d], "y", d) for d in (1, 2, 3)]
    gates = gate_proj.reshape(8, 2, n, dv)
    bases = residual.reshape(16, n, width)
    normed, ups, rows = [None, None], [None, None], [None, None]
    for k in (1, 0):
        shape = ((4, n, width), bf16)
        sources = (log, *incoming, within, scaled, gates)
        scratch = [pltpu.VMEM((dk, dv), bf16), pltpu.VMEM((tok // 2, dv), f32)]
        gated = ((tok // 2, dv), bf16)
        flops = tok * dv * width
        side = lambda own: functools.partial(heads_project_kernel, own=own)
        if k == 0:
            ready = run(functools.partial(gated_kernel, chunk=0), sc, sources, [gated], scratch=scratch, flops=flops)[0]
            send = run(side(False), sc, (ready, out_weight), [shape], flops=flops)[0]
        else:
            ready, send = run(
                functools.partial(heads_kernel, chunk=1), sc, (*sources, out_weight), [gated, shape],
                scratch=scratch, flops=flops,
            )
        keep = run(side(True), sc, (ready, out_weight), [shape], flops=flops)[0]
        normed[k] = reduce_and_norm(sc, keep, send, bases, norm_gain, norm_bias, 0, k)
        rows[k] = gather_rows(normed[k])
    ups[1], weights, down_weights = first_up(sc, rows[1], weights, 2 * hidden)
    ups[0] = second_up(sc, rows[0], weights, 2 * hidden)
    edge = lax.ppermute(ups[1][8 * n - 16 :], SP, [(i, i + 1) for i in range(15)])
    outs = [None, None]
    for k in (1, 0):
        keep, send = down_project(sc, ups[k], ups[1 - k], edge, taps, bias, down_weights, width, k)
        outs[k] = reduce_and_norm(sc, keep, send, normed[k][None], norm_gain, norm_bias, 1, None, *outs[k + 1 :])
    return outs[0]


def solution(mesh):
    torus = Mesh(mesh.devices.reshape(4, 4, 4, 2), SP + TP)
    return jax.shard_map(
        shards,
        mesh=torus,
        in_specs=(
            P(SP, TP),
            P(SP, TP),
            P(SP, TP),
            P(SP, TP),
            P(SP, TP),
            P(SP, None),
            P(TP, None),
            P(),
            P(),
            P(SP, TP),
            P(SP, TP),
            P(None, None, TP),
            P(None, TP),
            P(TP, SP),
        ),
        out_specs=P(SP + TP, None),
        check_vma=False,
    )
```
